512 devices in a mesh: sp: 64 (over z, y), tp: 8 (over x, core).
Axes of the slice: x: 4, y: 4, z: 16, core: 2. Of those that a mesh axis runs over, the one named last changes fastest.
Arguments:
- residual: bfloat16 [24576, 2048], P('sp'), may hold values from -6 to 6
- queries: bfloat16 [24576, 2048], P('sp', 'tp'), may hold values from -48 to 48
- keys: bfloat16 [24576, 2048], P('sp', 'tp'), may hold values from -48 to 48
- values: bfloat16 [24576, 2048], P('sp', 'tp'), may hold values from -6 to 6
- gate_cache: float32 [24576, 32], P('sp', 'tp'), may hold values from -6152 to 0, as said below
- doc_ids: int32 [24576], P('sp'), may hold values from 0 to 31, never falling along the last dimension, each value on 1 to 1536 neighbouring positions
- out_weight: bfloat16 [2048, 2048], P('tp'), may hold values from -1 to 1
- mix_gain: float32 [2048], replicated, may hold values from 0.1 to 1.9
- gate_weight: bfloat16 [2048, 5120], P('sp', 'tp'), may hold values from -0.125 to 0.125
- up_weight: bfloat16 [2048, 5120], P('sp', 'tp'), may hold values from -0.125 to 0.125
- down_weight: bfloat16 [5120, 2048], P('tp', 'sp'), may hold values from -0.15625 to 0.15625
Outputs:
- layer_out: bfloat16 [24576, 2048], P(('sp', 'tp'))
The draws below stay inside these ranges and needn't reach their ends.
Inputs may be any that keep to these rules, and one draw needn't show every extreme that they name: `doc_ids`: positions of one document are consecutive; each document has 1 to 1536 positions, and one has exactly that many. `gate_cache`: no column rises from one position to the next.
All inputs are finite; a program needn't handle non-finite values.
Results may differ from the reference program's by a relative error of at most 0.018.
Values may be sent and summed in bfloat16 or wider, within the bound.
A program may use at most 64 MiB of HBM per device.

```python
import math
import jax
import jax.numpy as jnp
import numpy as np
from jax import lax

D = 2048
HEAD_COUNT = 32
HEAD_DIM = 64
FF = 5120
REACH = 4
TOK_DEV = 384
TOKEN_COUNT = 24576
DOCS = 32
N_TP = 8


def drawn(key):
    base_key = jax.random.fold_in(key, 11)
    key_q, key_k = jax.random.split(base_key, 2)
    col_count = HEAD_COUNT * HEAD_DIM
    queries = jax.random.normal(key_q, (TOKEN_COUNT, col_count), jnp.float32)
    keys = jax.random.normal(key_k, (TOKEN_COUNT, col_count), jnp.float32)
    return (jnp.clip(queries, -48.0, 48.0), jnp.clip(keys, -48.0, 48.0))


def draw_queries(key, part):
    return drawn(key)[0].astype(jnp.bfloat16)


def draw_keys(key, part):
    return drawn(key)[1].astype(jnp.bfloat16)


def draw_gate_cache(key, part):
    base_key = jax.random.fold_in(key, 23)
    key_h, key_r, key_s, key_b, key_u, key_position, key_document = jax.random.split(base_key, 7)
    head_order = jax.random.permutation(key_h, HEAD_COUNT)
    slow_heads = head_order < HEAD_COUNT // 2
    fast_rate = jnp.exp(jax.random.uniform(key_r, (HEAD_COUNT,), jnp.float32, math.log(1.0 / 100.0), math.log(1.0 / 30.0)))
    slow_rate = jax.random.uniform(key_s, (HEAD_COUNT,), jnp.float32, 0.5, 2.0) / TOKEN_COUNT
    head_rate = jnp.where(slow_heads, slow_rate, fast_rate)
    blocks = TOKEN_COUNT // TOK_DEV
    factor = jnp.exp(jax.random.uniform(key_b, (blocks,), jnp.float32, math.log(0.4), math.log(2.5)))
    factor_rows = jnp.repeat(factor, TOK_DEV)
    wobble = jax.random.uniform(key_u, (TOKEN_COUNT, HEAD_COUNT), jnp.float32, 0.2, 1.8)
    logarithm_gate = -head_rate[None, :] * factor_rows[:, None] * wobble
    spike_start = jax.random.randint(key_position, (8,), 0, TOKEN_COUNT)
    spike_length = jnp.log(jax.random.uniform(key_document, (8, HEAD_COUNT), jnp.float32, 0.5, 0.8))
    logarithm_gate = logarithm_gate.at[spike_start].add(spike_length)
    return jnp.cumsum(logarithm_gate, axis=0)


def block_scale(stream_key, shape, cuts, least, largest):
    def one(position, parts):
        heights = jax.random.uniform(jax.random.fold_in(jax.random.fold_in(stream_key, 6), position), (parts,), jnp.float32, least / len(cuts), largest / len(cuts))
        return jnp.repeat(jnp.exp(heights), shape[position] // parts).reshape((-1,) + (1,) * (len(shape) - position - 1))

    loudness = one(*cuts[0])
    for cut in cuts[1:]:
        loudness = loudness * one(*cut)
    return loudness


def length_profile(amount, total, limit, slope):
    portions = [(1 << 20) // math.isqrt(rank ** slope) + 1 for rank in range(2, amount + 1)]
    surplus, given = total - limit - (amount - 1), [1] * (amount - 1)
    while surplus > 0:
        candidates = [i for i in range(amount - 1) if given[i] < limit]
        whole, remaining = sum([portions[i] for i in candidates]), surplus
        for i in candidates:
            addition = min(limit - given[i], max(1, remaining * portions[i] // whole), surplus)
            given[i] = given[i] + addition
            surplus = surplus - addition
    return np.array([limit] + given)


def ragged_sizes(rng, count, total, most, slope):
    if count == 2:
        one = jax.random.randint(rng, (), max(1, total - most), min(most, total - 1) + 1)
        return jnp.stack([one, total - one])
    tallies = jnp.asarray(length_profile(count, total, most, slope), jnp.int32)
    twos = (count - 1) // 2
    source_of, taker = tallies[1:1 + 2 * twos:2], tallies[2:2 + 2 * twos:2]
    margin = jnp.minimum(source_of - 1, most - taker)
    shifted = jax.random.randint(jax.random.fold_in(rng, 1), (twos,), 0, 1 << 20) % (margin + 1)
    tallies = tallies.at[1:1 + 2 * twos:2].set(source_of - shifted).at[2:2 + 2 * twos:2].set(taker + shifted)
    return tallies[jax.random.permutation(jax.random.fold_in(rng, 2), count)]


def noise(rng, dims, scale, reach, pieces=(), held_as=jnp.bfloat16):
    level = block_scale(rng, dims, pieces, -0.22, 0.18) if pieces else 1.0
    drawn = jax.random.normal(rng, dims, jnp.float32) * scale * level
    return jnp.minimum(jnp.maximum(drawn, -reach), reach).astype(held_as)


def setup_inputs(seed: int = 0) -> dict:
    streams_of = jax.random.split(jax.random.key(seed), 12)
    return {
        "residual": noise(streams_of[0], (TOKEN_COUNT, D), 1.0, 6.0, ((0, 64),)),
        "queries": draw_queries(jax.random.fold_in(streams_of[11], 71), 0),
        "keys": draw_keys(jax.random.fold_in(streams_of[11], 71), 0),
        "values": noise(streams_of[3], (TOKEN_COUNT, HEAD_COUNT * HEAD_DIM), 1.0, 6.0, ((0, 64), (1, 8))),
        "gate_cache": draw_gate_cache(jax.random.fold_in(streams_of[11], 71), 0),
        "doc_ids": jnp.searchsorted(jnp.cumsum(ragged_sizes(streams_of[5], DOCS, TOKEN_COUNT, REACH * TOK_DEV, 0)), jnp.arange(TOKEN_COUNT), side="right").astype(jnp.int32),
        "out_weight": noise(streams_of[6], (HEAD_COUNT * HEAD_DIM, D), (HEAD_COUNT * HEAD_DIM // 64) ** -0.5, 1.0, ((0, 8),)),
        "mix_gain": jnp.clip(1.0 + 0.18 * jax.random.normal(streams_of[7], (D,), jnp.float32), 0.1, 1.9),
        "gate_weight": noise(streams_of[8], (D, FF), D ** -0.5, 0.125, ((0, 64), (1, 8))),
        "up_weight": noise(streams_of[9], (D, FF), D ** -0.5, 0.125, ((0, 64), (1, 8))),
        "down_weight": noise(streams_of[10], (FF, D), (FF // 4) ** -0.5, 0.15625, ((0, 8), (1, 64))),
    }


EPSILON = 1e-06
NEGATIVE = -1e+30

def group_sum(activations, weight, groups):
    row_count = activations.shape[0]
    inner_cols = activations.shape[1] // groups
    left_grouped = activations.reshape(row_count, groups, inner_cols).transpose(1, 0, 2)
    right_grouped = weight.reshape(groups, inner_cols, weight.shape[1])

    def add_group(running, operands):
        partial_value = jnp.dot(operands[0], operands[1], preferred_element_type=jnp.float32)
        rounded = lax.optimization_barrier(partial_value.astype(jnp.bfloat16))
        return (running + rounded.astype(jnp.float32), None)
    zeros_init = jnp.zeros((row_count, weight.shape[1]), jnp.float32)
    running, ignored = lax.scan(add_group, zeros_init, (left_grouped, right_grouped))
    return running

def normalize(middle, gain):
    widened = middle.astype(jnp.float32)
    factor = lax.rsqrt(lax.optimization_barrier(jnp.mean(widened * widened, axis=-1, keepdims=True)) + EPSILON)
    return (widened * factor * gain).astype(jnp.bfloat16)

def attend(queries, keys, values, gate_cache, doc_ids):
    tokens = queries.shape[0]
    doc_span = REACH * TOK_DEV
    block_rows = math.gcd(tokens, 512)
    key_count = doc_span + block_rows
    head_shape = (tokens, HEAD_COUNT, HEAD_DIM)
    query_heads = queries.reshape(head_shape)
    pad_rows = ((doc_span, 0), (0, 0), (0, 0))
    key_heads = jnp.pad(keys.reshape(head_shape), pad_rows)
    value_heads = jnp.pad(values.reshape(head_shape), pad_rows)
    cache_pad = jnp.pad(gate_cache, ((doc_span, 0), (0, 0)))
    docs_pad = jnp.pad(doc_ids, (doc_span, 0), constant_values=-1)
    score_scale = HEAD_DIM ** (-0.5)

    def one_block(block_index):
        start_row = (block_index * block_rows).astype(jnp.int32)
        query_block = lax.dynamic_slice_in_dim(query_heads, start_row, block_rows, 0).astype(jnp.float32)
        key_block = lax.dynamic_slice_in_dim(key_heads, start_row, key_count, 0).astype(jnp.float32)
        value_block = lax.dynamic_slice_in_dim(value_heads, start_row, key_count, 0).astype(jnp.float32)
        query_cache = lax.dynamic_slice_in_dim(gate_cache, start_row, block_rows, 0)
        key_cache = lax.dynamic_slice_in_dim(cache_pad, start_row, key_count, 0)
        query_docs = lax.dynamic_slice_in_dim(doc_ids, start_row, block_rows, 0)
        key_docs = lax.dynamic_slice_in_dim(docs_pad, start_row, key_count, 0)
        query_pos = start_row + jnp.arange(block_rows, dtype=jnp.int32)
        key_pos = start_row - doc_span + jnp.arange(key_count, dtype=jnp.int32)
        visible = (key_pos[None, :] <= query_pos[:, None]) & (key_pos[None, :] >= 0) & (key_docs[None, :] == query_docs[:, None])
        scores = jnp.einsum('qhd,khd->hqk', query_block, key_block) * score_scale
        scores = scores + query_cache.T[:, :, None] - key_cache.T[:, None, :]
        scores = jnp.where(visible[None], scores, NEGATIVE)
        row_max = lax.optimization_barrier(jnp.max(scores, axis=-1, keepdims=True))
        exp_scores = jnp.exp(scores - row_max)
        weights = (exp_scores / lax.optimization_barrier(jnp.sum(exp_scores, axis=-1, keepdims=True))).astype(jnp.bfloat16)
        weights = lax.optimization_barrier(weights)
        mixed_out = jnp.einsum('hqk,khd->qhd', weights.astype(jnp.float32), value_block)
        return mixed_out.astype(jnp.bfloat16)
    blocks = lax.map(one_block, jnp.arange(tokens // block_rows, dtype=jnp.int32))
    return blocks.reshape(tokens, HEAD_COUNT * HEAD_DIM)

def reference(residual, queries, keys, values, gate_cache, doc_ids, out_weight, mix_gain, gate_weight, up_weight, down_weight):
    attended = attend(queries, keys, values, gate_cache, doc_ids)
    projected = group_sum(attended, out_weight, N_TP)
    middle = (residual.astype(jnp.float32) + projected).astype(jnp.bfloat16)
    normed = normalize(middle, mix_gain)
    gate_proj = jnp.dot(normed, gate_weight, preferred_element_type=jnp.float32)
    up_proj = jnp.dot(normed, up_weight, preferred_element_type=jnp.float32)
    hidden = (jax.nn.silu(gate_proj) * up_proj).astype(jnp.bfloat16)
    lowered = group_sum(hidden, down_weight, N_TP)
    return (middle.astype(jnp.float32) + lowered).astype(jnp.bfloat16)
```

```python
import functools
import math

import jax
import jax.numpy as jnp
from jax import lax
from jax.experimental import pallas as pl
from jax.experimental.pallas import tpu as pltpu
from jax.sharding import PartitionSpec as P

MESH = pl.DeviceIdType.MESH
EPSILON = 1e-06
NEGATIVE = -1e30
REACH = 4
NY = 4
LOG2E = math.log2(math.e)
F32 = jnp.float32
BF16 = jnp.bfloat16


def dot(a, b):
    return lax.dot_general(a, b, (((1,), (0,)), ((), ())), preferred_element_type=F32)


def dot_nt(a, b):
    return lax.dot_general(a, b, (((1,), (1,)), ((), ())), preferred_element_type=F32)


def kernel(
    n_sp, n_tp,
    q_ref, k_ref, v_ref, aux_ref, gu_ref, dt_ref, wo_ref, res_ref, gain_ref,
    out_ref,
    k_all, v_all, aux_all, gu, dt, wo, res, bias, att, part1, part2, pair1, pair2,
    stage, own, half1, half2, rs1, rs2, x_all, hidden, middle,
    loc, kv_s, kv_r, gz_s, gz_r, gy_s, gy_r, dy_s, dy_r, dz_s, dz_r, rs_s, rs_r, ag_s, ag_r,
):
    nz = n_sp // NY
    nx = n_tp // 2
    hz = nz // 2
    sp, tp = lax.axis_index("sp"), lax.axis_index("tp")
    z, y = sp // NY, sp % NY
    x, c = tp // 2, tp % 2
    tok, width = q_ref.shape
    heads = 4
    rows = tok // n_tp
    d_model = wo.shape[1]
    half = d_model // 2

    def at_sp(dz, dy):
        return ((z + dz + nz) % nz) * NY + (y + dy + NY) % NY

    def at_tp(dx, dc):
        return ((x + dx + nx) % nx) * 2 + (c + dc) % 2

    dev_z = ((at_sp(1, 0), tp), (at_sp(-1, 0), tp))
    dev_y = ((at_sp(0, 1), tp), (at_sp(0, -1), tp), (at_sp(0, 2), tp))
    dev_c = (sp, at_tp(0, 1))
    dev_x = ((sp, at_tp(1, 0)), (sp, at_tp(-1, 0)))

    def remote(src, dst, ssem, rsem, dev):
        return pltpu.make_async_remote_copy(
            src_ref=src, dst_ref=dst, send_sem=ssem, recv_sem=rsem, device_id=dev, device_id_type=MESH
        )

    last = REACH * tok
    local = [
        pltpu.make_async_copy(k_ref, k_all.at[pl.ds(last, tok)], loc.at[0]),
        pltpu.make_async_copy(v_ref, v_all.at[pl.ds(last, tok)], loc.at[1]),
        pltpu.make_async_copy(aux_ref, aux_all.at[:, pl.ds(last, tok)], loc.at[2]),
        pltpu.make_async_copy(gu_ref, gu.at[sp], loc.at[3]),
        pltpu.make_async_copy(dt_ref, dt.at[sp], loc.at[4]),
        pltpu.make_async_copy(wo_ref, wo, loc.at[5]),
        pltpu.make_async_copy(res_ref.at[pl.ds(pl.multiple_of(tp * rows, rows), rows)], res, loc.at[6]),
    ]
    for copy in local:
        copy.start()

    barrier = pltpu.get_barrier_semaphore()
    peers = (*dev_z, *dev_y, dev_c, *dev_x)
    for peer in peers:
        pl.semaphore_signal(barrier, inc=1, device_id=peer, device_id_type=MESH)
    pl.semaphore_wait(barrier, len(peers))

    def kv_slot(item, offset):
        if item == 2:
            return aux_all.at[:, pl.ds(pl.multiple_of(offset, 128), tok)]
        return (k_all, v_all)[item].at[pl.ds(pl.multiple_of(offset, 128), tok)]

    def kv_copy(item, kind, src, distance, dev):
        return remote(
            kv_slot(item, src), kv_slot(item, (REACH - distance) * tok),
            kv_s.at[item, kind], kv_r.at[item, distance - 1], dev,
        )

    def kv_prev(item):
        return kv_copy(item, 0, last, 4, dev_z[0])

    def kv_right(item, src):
        return kv_copy(item, 1, src, 1, dev_y[0])

    def kv_left(item, src):
        return kv_copy(item, 2, src, 3, dev_y[1])

    def kv_relay_right(item):
        return kv_copy(item, 3, (REACH - 1) * tok, 2, dev_y[0])

    def kv_relay_left(item):
        return kv_copy(item, 4, (REACH - 3) * tok, 2, dev_y[1])

    ITEMS = (2, 0, 1)
    for item in (2, 0, 1):
        local[item].wait()
        kv_prev(item).start()

        @pl.when(y < NY - 1)
        def _():
            kv_right(item, last).start()

        @pl.when(y == 0)
        def _():
            kv_left(item, last).start()

    def z_copy(way, r):
        shard = at_sp(-r, 0) if way == 0 else at_sp(r, 0)
        return remote(gu.at[shard], gu.at[shard], gz_s.at[way, r + 1], gz_r.at[way, r + 1], dev_z[way])

    def z_arrival(way, r):
        shard = at_sp(-r, 0) if way == 0 else at_sp(r, 0)
        return remote(gu.at[shard], gu.at[shard], gz_s.at[way, r], gz_r.at[way, r], dev_z[way])

    def y_copy(way, o):
        shard, plane = at_sp(o, 0), (o + nz) % nz
        return remote(gu.at[shard], gu.at[shard], gy_s.at[way, plane], gy_r.at[way, plane], dev_y[way])

    def y_arrival(way, o):
        shard, plane = at_sp(o, -1 if way == 0 else 1), (o + nz) % nz
        return remote(gu.at[shard], gu.at[shard], gy_s.at[way, plane], gy_r.at[way, plane], dev_y[way])

    def y_forward(way, o):
        shard, plane = at_sp(o, -1 if way == 0 else 1), (o + nz) % nz
        return remote(gu.at[shard], gu.at[shard], gy_s.at[2, plane], gy_r.at[2, plane], dev_y[way])

    def y_across(o):
        shard, plane = at_sp(o, 2), (o + nz) % nz
        return remote(gu.at[shard], gu.at[shard], gy_s.at[2, plane], gy_r.at[2, plane], dev_y[0])

    def d_copy(i):
        return remote(dt.at[sp], dt.at[sp], dy_s.at[i], dy_r.at[i], dev_y[i])

    def d_arrival(i):
        shard = at_sp(0, (-1, 1, 2)[i])
        return remote(dt.at[shard], dt.at[shard], dy_s.at[i], dy_r.at[i], dev_y[i])

    def q_ref_of(way, r):
        plane = (z + (-r if way == 0 else r) + nz) % nz
        return dt.at[pl.ds(plane * NY, NY)]

    def q_copy(way, r):
        block = q_ref_of(way, r)
        return remote(block, block, dz_s.at[way, r + 1], dz_r.at[way, r + 1], dev_z[way])

    def q_arrival(way, r):
        block = q_ref_of(way, r)
        return remote(block, block, dz_s.at[way, r], dz_r.at[way, r], dev_z[way])

    def z_round(r, at_end=0):
        z_arrival(0, r).wait_recv()
        if at_end < 2:
            z_copy(0, r).start()
        y_copy(0, -r).start()
        y_copy(1, -r).start()
        if at_end < 2:
            z_arrival(1, r).wait_recv()
            if at_end < 1:
                z_copy(1, r).start()
            y_copy(0, r).start()
            y_copy(1, r).start()

    def y_round(r, at_end=0):
        if at_end < 2:
            y_arrival(1, r).wait_recv()
            y_forward(1, r).start()
        if not (isinstance(r, int) and r == 0):
            y_arrival(0, -r).wait_recv()
            y_forward(0, -r).start()

    def q_round(r, at_end=0):
        q_arrival(0, r).wait_recv()
        if at_end < 2:
            q_copy(0, r).start()
            q_arrival(1, r).wait_recv()
            if at_end < 1:
                q_copy(1, r).start()

    def stage_of(r):
        return 2 if r == hz else 1 if r == hz - 1 else 0

    def full_round(r):
        z_round(r, stage_of(r))
        y_round(r - 1, stage_of(r - 1))
        q_round(r, stage_of(r))

    local[3].wait()
    z_copy(0, 0).start()
    z_copy(1, 0).start()
    y_copy(0, 0).start()
    y_copy(1, 0).start()
    local[4].wait()
    for i in range(3):
        d_copy(i).start()

    for item in ITEMS:
        kv_copy(item, 0, last, 4, dev_z[0]).wait_recv()

        @pl.when(y == NY - 1)
        def _():
            kv_right(item, 0).start()

        @pl.when(y > 0)
        def _():
            kv_left(item, 0).start()

    for i in range(3):
        d_arrival(i).wait_recv()
    q_copy(0, 0).start()
    q_copy(1, 0).start()

    for item in ITEMS:
        kv_right(item, last).wait_recv()

        @pl.when((y == 1) | (y == 2))
        def _():
            kv_relay_right(item).start()

        kv_left(item, last).wait_recv()

        @pl.when((y == 1) | (y == 2))
        def _():
            kv_relay_left(item).start()

    full_round(1)
    for item in ITEMS:
        kv_relay_right(item).wait_recv()

    tile = 128 if tok % 128 == 0 else tok
    window = REACH * tok + tile
    lanes = lax.broadcasted_iota(jnp.int32, (1, width), 1) // (width // heads)
    scale = (width // heads) ** -0.5 * LOG2E
    own_docs = jnp.transpose(aux_all[:, pl.ds(last, tok)], (1, 0))
    att_docs = own_docs[:, heads : heads + 1]
    origin = own_docs[0:1, 0:heads]
    half1[...] = jnp.broadcast_to(att_docs, half1.shape)

    def attend(i, carry):
        start = pl.multiple_of(i * tile, tile)
        doc_row = aux_all[heads : heads + 1, pl.ds(start, window)]
        doc_col = half1[pl.ds(start, tile), 0:1]
        gap = lax.broadcasted_iota(jnp.int32, (tile, window), 1) - lax.broadcasted_iota(jnp.int32, (tile, window), 0)
        bias[...] = jnp.where((doc_row == doc_col) & (gap <= REACH * tok), 0.0, NEGATIVE)
        queries = q_ref[pl.ds(start, tile), :]
        keys = k_all[pl.ds(start, window), :]
        values = v_all[pl.ds(start, window), :]
        total = jnp.zeros((tile, width), F32)
        for h in range(heads):
            masked = jnp.where(lanes == h, queries, jnp.zeros_like(queries))
            gates = (origin[:, h : h + 1] - aux_all[h : h + 1, pl.ds(start, window)]) * LOG2E
            scores = dot_nt(masked, keys) * scale + gates + bias[...]
            peak = jnp.max(scores, axis=-1, keepdims=True)
            weights = jnp.exp2(scores - peak)
            norm = jnp.sum(weights, axis=-1, keepdims=True)
            mixed = dot(weights.astype(BF16), values)
            total = jnp.where(lanes == h, mixed / norm, total)
        att[pl.ds(start, tile), :] = total.astype(BF16)
        r = i + 2
        z_round(r)
        y_round(r - 1)
        q_round(r)
        return carry

    n_tiles = tok // tile
    lax.fori_loop(0, n_tiles, attend, 0)
    rounds = [functools.partial(full_round, r) for r in range(n_tiles + 2, hz + 1)]

    def serve():
        if rounds:
            rounds.pop(0)()

    n_tile = 256

    def summed(part, pair, half_in, rs_in, k, service):
        swap = remote(part.at[:, 1 - c], pair, rs_s.at[k, 0], rs_r.at[k, 0], dev_c)
        swap.start()
        service()
        swap.wait_recv()

        def on_chip(there):
            return part[there, c].astype(F32) + pair[there].astype(F32)

        far, right, left = (x + 2) % nx, (x + 1) % nx, (x + nx - 1) % nx
        lo, hi = pl.ds(0, half), pl.ds(half, half)
        total = on_chip(far).astype(BF16)
        stage[k, 0] = total[:, :half]
        stage[k, 1] = total[:, half:]
        first = [
            remote(stage.at[k, 0], half_in.at[0], rs_s.at[k, 1], rs_r.at[k, 1], dev_x[0]),
            remote(stage.at[k, 1], half_in.at[1], rs_s.at[k, 2], rs_r.at[k, 2], dev_x[1]),
        ]
        first[0].start()
        first[1].start()
        to_right = on_chip(right)
        to_left = on_chip(left)
        stage[k, 2] = to_right[:, half:].astype(BF16)
        stage[k, 3] = to_left[:, :half].astype(BF16)
        second = [
            remote(stage.at[k, 2], rs_in.at[0, 1], rs_s.at[k, 3], rs_r.at[k, 3], dev_x[0]),
            remote(stage.at[k, 3], rs_in.at[1, 0], rs_s.at[k, 4], rs_r.at[k, 4], dev_x[1]),
        ]
        second[0].start()
        second[1].start()
        own[...] = on_chip(x)
        service()
        first[0].wait_recv()
        stage[k, 4] = (to_right[:, :half] + half_in[0].astype(F32)).astype(BF16)
        third = remote(stage.at[k, 4], rs_in.at[0, 0], rs_s.at[k, 5], rs_r.at[k, 5], dev_x[0])
        third.start()
        first[1].wait_recv()
        stage[k, 5] = (to_left[:, half:] + half_in[1].astype(F32)).astype(BF16)
        fourth = remote(stage.at[k, 5], rs_in.at[1, 1], rs_s.at[k, 6], rs_r.at[k, 6], dev_x[1])
        fourth.start()
        for copy in (*second, third, fourth):
            copy.wait_recv()
        sends = (swap, *first, *second, third, fourth)
        halves = [
            own[:, i * half : (i + 1) * half] + rs_in[0, i].astype(F32) + rs_in[1, i].astype(F32) for i in range(2)
        ]
        return jnp.concatenate(halves, axis=-1), sends

    local[5].wait()
    attended = att[...]

    def project(n, carry):
        cols = pl.ds(pl.multiple_of(n * n_tile, n_tile), n_tile)
        product = dot(attended, wo[:, cols]).astype(BF16)
        part1[:, :, :, cols] = product.reshape(nx, 2, rows, n_tile)
        return carry

    lax.fori_loop(0, d_model // n_tile, project, 0)
    attn_sum, sends1 = summed(part1, pair1, half2.at[0], rs1, 0, serve)
    local[6].wait()
    mid = (res[...].astype(F32) + attn_sum).astype(BF16)
    middle[...] = mid
    wide = mid.astype(F32)
    factor = lax.rsqrt(jnp.mean(wide * wide, axis=-1, keepdims=True) + EPSILON)
    x_all[tp] = (wide * factor * gain_ref[...]).astype(BF16)

    def ag(slot, cols, i, dev):
        ref = x_all.at[slot] if cols is None else x_all.at[slot, :, cols]
        return remote(ref, ref, ag_s.at[i], ag_r.at[i], dev)

    lo, hi = pl.ds(0, half), pl.ds(half, half)
    sends2 = [ag(tp, None, 0, dev_x[0]), ag(tp, None, 1, dev_x[1]), ag(tp, None, 4, dev_c)]
    for copy in sends2:
        copy.start()
    serve()
    from_left, from_right, from_far = at_tp(-1, 0), at_tp(1, 0), at_tp(2, 0)
    ag(from_left, None, 0, dev_x[0]).wait_recv()
    more = [ag(from_left, lo, 2, dev_x[0]), ag(from_left, None, 5, dev_c)]
    for copy in more:
        copy.start()
    sends2 += more
    ag(from_right, None, 1, dev_x[1]).wait_recv()
    more = [ag(from_right, hi, 3, dev_x[1]), ag(from_right, None, 6, dev_c)]
    for copy in more:
        copy.start()
    sends2 += more
    ag(from_far, lo, 2, dev_x[0]).wait_recv()
    ag(from_far, hi, 3, dev_x[1]).wait_recv()
    copy = ag(from_far, None, 7, dev_c)
    copy.start()
    sends2.append(copy)
    while rounds:
        serve()
    y_round(hz, 2)
    ag(at_tp(0, 1), None, 4, dev_c).wait_recv()
    ag(at_tp(-1, 1), None, 5, dev_c).wait_recv()
    ag(at_tp(1, 1), None, 6, dev_c).wait_recv()
    ag(at_tp(2, 1), None, 7, dev_c).wait_recv()

    def rest(o, carry):
        y_arrival(0, o).wait_recv()
        y_across(o).wait_recv()
        y_arrival(1, o - hz).wait_recv()
        y_across(o - hz).wait_recv()
        return carry

    lax.fori_loop(0, hz, rest, 0)

    ff = hidden.shape[1]

    def expand(n, carry):
        cols = pl.ds(pl.multiple_of(n * 256, 256), 256)
        both = dot(x_all[...].reshape(tok, d_model), gu[:, :, cols].reshape(d_model, 256))
        gate, up = both[:, :128], both[:, 128:]
        act = gate / (1.0 + jnp.exp(-gate)) * up
        hidden[:, pl.ds(pl.multiple_of(n * 128, 128), 128)] = act.astype(BF16)
        return carry

    lax.fori_loop(0, ff // 128, expand, 0)
    group = n_tile // (d_model // n_sp)

    def contract(n, carry):
        cols = pl.ds(pl.multiple_of(n * n_tile, n_tile), n_tile)
        block = dt[pl.ds(n * group, group)].reshape(n_tile, ff)
        product = dot_nt(hidden[...], block).astype(BF16)
        part2[:, :, :, cols] = product.reshape(nx, 2, rows, n_tile)
        return carry

    lax.fori_loop(0, d_model // n_tile, contract, 0)
    down_sum, sends3 = summed(part2, pair2, half2.at[1], rs2, 1, lambda: None)
    out_ref[...] = (middle[...].astype(F32) + down_sum).astype(BF16)

    for copy in (*sends1, *sends2, *sends3):
        copy.wait_send()
    for item in ITEMS:
        kv_prev(item).wait_send()
        kv_right(item, last).wait_send()
        kv_left(item, last).wait_send()

        @pl.when((y == 1) | (y == 2))
        def _():
            kv_relay_right(item).wait_send()
            kv_relay_left(item).wait_send()

    for i in range(3):
        d_copy(i).wait_send()

    def gone_z(r, carry):
        for way in range(2):
            z_copy(way, r).wait_send()
            q_copy(way, r).wait_send()
        return carry

    lax.fori_loop(0, hz - 1, gone_z, 0)
    z_copy(0, hz - 1).wait_send()
    q_copy(0, hz - 1).wait_send()

    def gone_y(o, carry):
        y_copy(0, o).wait_send()
        y_copy(1, o).wait_send()
        y_across(o).wait_send()
        return carry

    lax.fori_loop(0, nz, gone_y, 0)


def local(n_sp, n_tp, residual, queries, keys, values, gate_cache, doc_ids, out_weight, mix_gain, gate_weight, up_weight, down_weight):
    tok, width = queries.shape
    d_model = out_weight.shape[1]
    rows = tok // n_tp
    wr, ff = gate_weight.shape
    heads = gate_cache.shape[1]
    both = jnp.concatenate(
        [gate_weight.reshape(wr, ff // 128, 1, 128), up_weight.reshape(wr, ff // 128, 1, 128)], axis=2
    ).reshape(wr, 2 * ff)
    down = down_weight.T
    aux = jnp.concatenate(
        [gate_cache.T, doc_ids.astype(F32)[None], jnp.zeros((8 - heads - 1, tok), F32)], axis=0
    )
    nz = n_sp // NY
    hz = nz // 2
    tile = 128 if tok % 128 == 0 else tok
    half = d_model // 2
    vmem = pl.BlockSpec(memory_space=pltpu.VMEM)
    anywhere = pl.BlockSpec(memory_space=pl.ANY)
    dma = pltpu.SemaphoreType.DMA
    return pl.pallas_call(
        functools.partial(kernel, n_sp, n_tp),
        out_shape=jax.ShapeDtypeStruct((rows, d_model), BF16),
        in_specs=[vmem, anywhere, anywhere, anywhere, anywhere, anywhere, anywhere, anywhere, vmem],
        out_specs=vmem,
        scratch_shapes=[
            pltpu.VMEM(((REACH + 1) * tok, width), BF16),
            pltpu.VMEM(((REACH + 1) * tok, width), BF16),
            pltpu.VMEM((8, (REACH + 1) * tok), F32),
            pltpu.VMEM((n_sp, wr, 2 * ff), BF16),
            pltpu.VMEM((n_sp, wr, ff), BF16),
            pltpu.VMEM((width, d_model), BF16),
            pltpu.VMEM((rows, d_model), BF16),
            pltpu.VMEM((tile, REACH * tok + tile), F32),
            pltpu.VMEM((tok, width), BF16),
            pltpu.VMEM((n_tp // 2, 2, rows, d_model), BF16),
            pltpu.VMEM((n_tp // 2, 2, rows, d_model), BF16),
            pltpu.VMEM((n_tp // 2, rows, d_model), BF16),
            pltpu.VMEM((n_tp // 2, rows, d_model), BF16),
            pltpu.VMEM((2, 6, rows, half), BF16),
            pltpu.VMEM((rows, d_model), F32),
            pltpu.VMEM((tok, 128), F32),
            pltpu.VMEM((2, 2, rows, half), BF16),
            pltpu.VMEM((2, 2, rows, half), BF16),
            pltpu.VMEM((2, 2, rows, half), BF16),
            pltpu.VMEM((n_tp, rows, d_model), BF16),
            pltpu.VMEM((tok, ff), BF16),
            pltpu.VMEM((rows, d_model), BF16),
            dma((7,)),
            dma((3, 5)),
            dma((3, 4)),
            dma((2, hz + 1)),
            dma((2, hz + 1)),
            dma((3, nz)),
            dma((3, nz)),
            dma((3,)),
            dma((3,)),
            dma((2, hz + 1)),
            dma((2, hz + 1)),
            dma((2, 7)),
            dma((2, 7)),
            dma((8,)),
            dma((8,)),
        ],
        compiler_params=pltpu.CompilerParams(
            collective_id=0, has_side_effects=True, vmem_limit_bytes=60 * 1024 * 1024
        ),
    )(queries, keys, values, aux, both, down, out_weight, residual, mix_gain[None])


def solution(mesh):
    n_sp, n_tp = mesh.shape["sp"], mesh.shape["tp"]
    return jax.shard_map(
        functools.partial(local, n_sp, n_tp),
        mesh=mesh,
        in_specs=(
            P("sp", None), P("sp", "tp"), P("sp", "tp"), P("sp", "tp"), P("sp", "tp"), P("sp"),
            P("tp", None), P(), P("sp", "tp"), P("sp", "tp"), P("tp", "sp"),
        ),
        out_specs=P(("sp", "tp"), None),
        check_vma=False,
    )
```

```python
import functools
import math

import jax
import jax.numpy as jnp
from jax import lax
from jax.experimental import pallas as pl
from jax.experimental.pallas import tpu as pltpu
from jax.sharding import PartitionSpec as P

MESH = pl.DeviceIdType.MESH
EPSILON = 1e-06
NEGATIVE = -1e30
REACH = 4
NY = 4
LOG2E = math.log2(math.e)
F32 = jnp.float32
BF16 = jnp.bfloat16


def dot(a, b):
    return lax.dot_general(a, b, (((1,), (0,)), ((), ())), preferred_element_type=F32)


def dot_nt(a, b):
    return lax.dot_general(a, b, (((1,), (1,)), ((), ())), preferred_element_type=F32)


def kernel(
    n_sp, n_tp,
    q_ref, k_ref, v_ref, aux_ref, p_ref, d_ref, wo_ref, res_ref, gain_ref,
    out_ref,
    k_all, v_all, aux_all, gu, qd, wo, res, bias, doc_col, att, part, pair,
    stage, own, half_in, rs_in, x_all, hidden, middle,
    loc, kv_s, kv_r, gz_s, gz_r, gy_s, gy_r, dy_s, dy_r, dz_s, dz_r, rs_s, rs_r, wo_s, wo_r, ag_s, ag_r,
):
    nz = n_sp // NY
    nx = n_tp // 2
    hz = nz // 2
    sp, tp = lax.axis_index("sp"), lax.axis_index("tp")
    z, y = sp // NY, sp % NY
    x, c = tp // 2, tp % 2
    tok, width = q_ref.shape
    heads = 4
    rows = tok // n_tp
    d_model = wo.shape[2]
    half = d_model // 2
    ff = hidden.shape[1]
    extra = qd.shape[2] - ff
    tile = 128
    n_tiles = tok // tile

    def at_sp(dz, dy):
        return ((z + dz + nz) % nz) * NY + (y + dy + NY) % NY

    def at_tp(dx, dc):
        return ((x + dx + nx) % nx) * 2 + (c + dc) % 2

    dev_z = ((at_sp(1, 0), tp), (at_sp(-1, 0), tp))
    dev_y = ((at_sp(0, 1), tp), (at_sp(0, -1), tp), (at_sp(0, 2), tp))
    dev_c = (sp, at_tp(0, 1))
    dev_x = ((sp, at_tp(1, 0)), (sp, at_tp(-1, 0)))

    def remote(src, dst, ssem, rsem, dev):
        return pltpu.make_async_remote_copy(
            src_ref=src, dst_ref=dst, send_sem=ssem, recv_sem=rsem, device_id=dev, device_id_type=MESH
        )

    last = REACH * tok
    local = [
        pltpu.make_async_copy(k_ref, k_all.at[pl.ds(last, tok)], loc.at[0]),
        pltpu.make_async_copy(v_ref, v_all.at[pl.ds(last, tok)], loc.at[1]),
        pltpu.make_async_copy(aux_ref, aux_all.at[:, pl.ds(last, tok)], loc.at[2]),
        pltpu.make_async_copy(p_ref, gu.at[sp], loc.at[3]),
        pltpu.make_async_copy(d_ref, qd.at[sp], loc.at[4]),
        pltpu.make_async_copy(wo_ref, wo.at[tp], loc.at[5]),
        pltpu.make_async_copy(res_ref, res, loc.at[6]),
    ]
    for i in (4, 2, 0, 1, 3, 5, 6):
        local[i].start()

    barrier = pltpu.get_barrier_semaphore()
    peers = (*dev_z, *dev_y, dev_c, *dev_x)
    for peer in peers:
        pl.semaphore_signal(barrier, inc=1, device_id=peer, device_id_type=MESH)
    pl.semaphore_wait(barrier, len(peers))

    def kv_slot(item, offset):
        if item == 2:
            return aux_all.at[:, pl.ds(pl.multiple_of(offset, 128), tok)]
        return (k_all, v_all)[item].at[pl.ds(pl.multiple_of(offset, 128), tok)]

    def kv_copy(item, kind, src, distance, dev):
        return remote(
            kv_slot(item, src), kv_slot(item, (REACH - distance) * tok),
            kv_s.at[item, kind], kv_r.at[item, distance - 1], dev,
        )

    def kv_prev(item):
        return kv_copy(item, 0, last, 4, dev_z[0])

    def kv_right(item, src):
        return kv_copy(item, 1, src, 1, dev_y[0])

    def kv_left(item, src):
        return kv_copy(item, 2, src, 3, dev_y[1])

    def kv_relay_right(item):
        return kv_copy(item, 3, (REACH - 1) * tok, 2, dev_y[0])

    def kv_relay_left(item):
        return kv_copy(item, 4, (REACH - 3) * tok, 2, dev_y[1])

    ITEMS = (2, 0, 1)

    def kv_own(item):
        local[item].wait()
        kv_prev(item).start()

        @pl.when(y < NY - 1)
        def _():
            kv_right(item, last).start()

        @pl.when(y == 0)
        def _():
            kv_left(item, last).start()

    def kv_turn(item):
        kv_prev(item).wait_recv()

        @pl.when(y == NY - 1)
        def _():
            kv_right(item, 0).start()

        @pl.when(y > 0)
        def _():
            kv_left(item, 0).start()

    def kv_relay(item):
        kv_right(item, last).wait_recv()

        @pl.when((y == 1) | (y == 2))
        def _():
            kv_relay_right(item).start()

        kv_left(item, last).wait_recv()

        @pl.when((y == 1) | (y == 2))
        def _():
            kv_relay_left(item).start()

    def z_copy(way, r):
        shard = at_sp(-r, 0) if way == 0 else at_sp(r, 0)
        return remote(gu.at[shard], gu.at[shard], gz_s.at[way, r + 1], gz_r.at[way, r + 1], dev_z[way])

    def z_arrival(way, r):
        shard = at_sp(-r, 0) if way == 0 else at_sp(r, 0)
        return remote(gu.at[shard], gu.at[shard], gz_s.at[way, r], gz_r.at[way, r], dev_z[way])

    def y_move(way, o, dy, lane):
        shard, plane = at_sp(o, dy), (o + nz) % nz
        return remote(gu.at[shard], gu.at[shard], gy_s.at[lane, plane], gy_r.at[lane, plane], dev_y[way])

    def y_copy(way, o):
        return y_move(way, o, 0, way)

    def y_arrival(way, o):
        return y_move(way, o, -1 if way == 0 else 1, way)

    def y_forward(way, o):
        return y_move(way, o, -1 if way == 0 else 1, 2)

    def y_across(o):
        return y_move(0, o, 2, 2)

    def d_copy(i):
        return remote(qd.at[sp], qd.at[sp], dy_s.at[i], dy_r.at[i], dev_y[i])

    def d_arrival(i):
        shard = at_sp(0, (-1, 1, 2)[i])
        return remote(qd.at[shard], qd.at[shard], dy_s.at[i], dy_r.at[i], dev_y[i])

    def q_move(way, r, s, step):
        plane = (z + (-r if way == 0 else r) + nz) % nz
        block = qd.at[pl.ds(plane * NY + s * (NY // 2), NY // 2)]
        return remote(block, block, dz_s.at[way, r + step, s], dz_r.at[way, r + step, s], dev_z[way])

    def q_copy(way, r, s):
        return q_move(way, r, s, 1)

    def q_arrival(way, r, s):
        return q_move(way, r, s, 0)

    def pieces(r):
        fixed = isinstance(r, int)

        def along_z():
            for way in range(2):
                count = hz - 1 + way
                if fixed and r > count:
                    continue
                z_arrival(way, r).wait_recv()
                if not fixed or r < count:
                    z_copy(way, r).start()
                for side in range(2):
                    y_copy(side, -r if way == 0 else r).start()

        def bundles(s):
            for way in range(2):
                count = hz - 1 + way
                if fixed and r > count:
                    continue
                q_arrival(way, r, s).wait_recv()
                if not fixed or r < count:
                    q_copy(way, r, s).start()

        def along_y():
            y_turn(r - 1)

        return [along_z, functools.partial(bundles, 0), along_y, functools.partial(bundles, 1)]

    def y_turn(r):
        fixed = isinstance(r, int)
        if not fixed or r < hz:
            y_arrival(0, -r).wait_recv()
            y_forward(0, -r).start()
        if not fixed or r > 0:
            y_arrival(1, r).wait_recv()
            y_forward(1, r).start()

    class Gather:
        def __init__(self, view, send, recv, count):
            self.view, self.send, self.recv, self.count = view, send, recv, count

        def copy(self, kind, slot, j):
            ref = self.view(slot, j, {2: 0, 3: 1}.get(kind))
            dev = dev_c if kind >= 4 else dev_x[kind % 2]
            return remote(ref, ref, self.send.at[kind, j], self.recv.at[kind, j], dev)

        def begin(self, j):
            for kind in (0, 1, 4):
                self.copy(kind, tp, j).start()

        def near(self, j):
            for way in range(2):
                slot = at_tp(2 * way - 1, 0)
                self.copy(way, slot, j).wait_recv()
                self.copy(2 + way, slot, j).start()
                self.copy(5 + way, slot, j).start()

        def far(self, j):
            slot = at_tp(2, 0)
            self.copy(2, slot, j).wait_recv()
            self.copy(3, slot, j).wait_recv()
            self.copy(7, slot, j).start()

        def done(self, j):
            for kind, dx in ((4, 0), (5, -1), (6, 1), (7, 2)):
                self.copy(kind, at_tp(dx, 1), j).wait_recv()

        def gone(self):
            for kind in range(8):
                for j in range(self.count):
                    self.copy(kind, tp, j).wait_send()

    def wo_view(slot, j, part_of):
        size = width // 4
        if part_of is None:
            return wo.at[slot, pl.ds(j * size, size)]
        return wo.at[slot, pl.ds(j * size + part_of * (size // 2), size // 2)]

    def att_view(slot, j, part_of):
        cols = pl.ds(pl.multiple_of(slot * width, 128), width)
        if part_of is None:
            return att.at[pl.ds(pl.multiple_of(j * tile, tile), tile), cols]
        return att.at[pl.ds(pl.multiple_of(j * tile + part_of * (tile // 2), tile // 2), tile // 2), cols]

    wos = Gather(wo_view, wo_s, wo_r, 4)
    ats = Gather(att_view, ag_s, ag_r, n_tiles)

    local[4].wait()
    for i in range(3):
        d_copy(i).start()
    for item in ITEMS:
        kv_own(item)
    local[3].wait()
    z_copy(0, 0).start()
    z_copy(1, 0).start()
    y_copy(0, 0).start()
    y_copy(1, 0).start()
    local[5].wait()
    for j in range(4):
        wos.begin(j)
    for i in range(3):
        d_arrival(i).wait_recv()
    for s in range(2):
        for way in range(2):
            q_copy(way, 0, s).start()
    kv_turn(2)
    kv_turn(0)
    wos.near(0)
    kv_turn(1)
    kv_relay(2)
    kv_relay(0)
    wos.near(1)
    first = pieces(1)
    first[0]()
    kv_relay(1)
    for piece in first[1:]:
        piece()
    wos.near(2)
    for piece in pieces(2):
        piece()
    wos.near(3)
    for item in ITEMS:
        kv_relay_right(item).wait_recv()

    window = REACH * tok + tile
    lanes = lax.broadcasted_iota(jnp.int32, (1, width), 1) // (width // heads)
    scale = (width // heads) ** -0.5 * LOG2E
    own_docs = jnp.transpose(aux_all[:, pl.ds(last, tok)], (1, 0))
    origin = own_docs[0:1, 0:heads]
    doc_col[...] = jnp.broadcast_to(own_docs[:, heads : heads + 1], doc_col.shape)
    own_cols = pl.ds(pl.multiple_of(tp * width, 128), width)

    def attend(i, carry):
        start = pl.multiple_of(i * tile, tile)
        doc_row = aux_all[heads : heads + 1, pl.ds(start, window)]
        doc_here = doc_col[pl.ds(start, tile), 0:1]
        gap = lax.broadcasted_iota(jnp.int32, (tile, window), 1) - lax.broadcasted_iota(jnp.int32, (tile, window), 0)
        bias[...] = jnp.where((doc_row == doc_here) & (gap <= REACH * tok), 0.0, NEGATIVE)
        queries = q_ref[pl.ds(start, tile), :]
        keys = k_all[pl.ds(start, window), :]
        values = v_all[pl.ds(start, window), :]
        total = jnp.zeros((tile, width), F32)
        service = pieces(i + 3)
        for h in range(heads):
            masked = jnp.where(lanes == h, queries, jnp.zeros_like(queries))
            gates = (origin[:, h : h + 1] - aux_all[h : h + 1, pl.ds(start, window)]) * LOG2E
            scores = dot_nt(masked, keys) * scale + gates + bias[...]
            peak = jnp.max(scores, axis=-1, keepdims=True)
            weights = jnp.exp2(scores - peak)
            norm = jnp.sum(weights, axis=-1, keepdims=True)
            mixed = dot(weights.astype(BF16), values)
            total = jnp.where(lanes == h, mixed / norm, total)
            if h == heads - 1:
                att[pl.ds(start, tile), own_cols] = total.astype(BF16)
                ats.begin(i)

            @pl.when(i < n_tiles - 1)
            def _():
                service[h]()

        wos.far(i)

        @pl.when(i >= 1)
        def _():
            ats.near(i - 1)

        return carry

    lax.fori_loop(0, n_tiles, attend, 0)
    queue = [piece for r in range(n_tiles + 2, hz + 1) for piece in pieces(r)]

    def serve(count):
        for _ in range(min(count, len(queue))):
            queue.pop(0)()

    n_tile = 256

    def project(i):
        block = pl.ds(i * tile, tile)

        def columns(n, carry):
            cols = pl.ds(pl.multiple_of(n * n_tile, n_tile), n_tile)
            product = dot(att[block, :], wo[:, :, cols].reshape(n_tp * width, n_tile))
            middle[block, cols] = (res[block, cols].astype(F32) + product).astype(BF16)
            return carry

        lax.fori_loop(0, d_model // n_tile, columns, 0)
        wide = middle[block, :].astype(F32)
        factor = lax.rsqrt(jnp.mean(wide * wide, axis=-1, keepdims=True) + EPSILON)
        x_all[block, :] = (wide * factor * gain_ref[...]).astype(BF16)

    ats.far(0)
    wos.far(3)
    ats.near(2)
    serve(2)
    for j in range(4):
        wos.done(j)
    ats.done(0)
    local[6].wait()
    project(0)
    serve(2)
    ats.far(1)
    ats.far(2)
    ats.done(1)
    project(1)
    serve(4)
    ats.done(2)
    project(2)
    serve(len(queue))
    y_turn(hz)

    def rest(r, carry):
        y_arrival(1, -r).wait_recv()
        y_across(-r).wait_recv()
        y_arrival(0, r + 1).wait_recv()
        y_across(r + 1).wait_recv()
        return carry

    lax.fori_loop(0, hz, rest, 0)

    def activate(both, n):
        gate, up = both[:, :128], both[:, 128:]
        hidden[:, pl.ds(pl.multiple_of(n * 128, 128), 128)] = (gate / (1.0 + jnp.exp(-gate)) * up).astype(BF16)

    def expand(n, carry):
        cols = pl.ds(pl.multiple_of(n * 256, 256), 256)
        activate(dot(x_all[...], gu[:, :, cols].reshape(d_model, 256)), n)
        return carry

    lax.fori_loop(0, gu.shape[2] // 256, expand, 0)
    for n in range(extra // 256):
        activate(dot(x_all[...], qd[:, :, n * 256 : (n + 1) * 256].reshape(d_model, 256)), gu.shape[2] // 256 + n)
    group = n_tile // (d_model // n_sp)

    def contract(n, carry):
        cols = pl.ds(pl.multiple_of(n * n_tile, n_tile), n_tile)
        block = qd[pl.ds(n * group, group), :, extra:].reshape(n_tile, ff)
        product = dot_nt(hidden[...], block).astype(BF16)
        part[:, :, :, cols] = product.reshape(nx, 2, rows, n_tile)
        return carry

    lax.fori_loop(0, d_model // n_tile, contract, 0)

    swap = remote(part.at[:, 1 - c], pair, rs_s.at[0], rs_r.at[0], dev_c)
    swap.start()
    swap.wait_recv()

    def on_chip(there):
        return part[there, c].astype(F32) + pair[there].astype(F32)

    opposite, right, left = (x + 2) % nx, (x + 1) % nx, (x + nx - 1) % nx
    total = on_chip(opposite).astype(BF16)
    stage[0] = total[:, :half]
    stage[1] = total[:, half:]
    sends = [swap]

    def send(i, dst, way):
        copy = remote(stage.at[i], dst, rs_s.at[i + 1], rs_r.at[i + 1], dev_x[way])
        copy.start()
        sends.append(copy)
        return copy

    first = send(0, half_in.at[0], 0), send(1, half_in.at[1], 1)
    to_right = on_chip(right)
    to_left = on_chip(left)
    stage[2] = to_right[:, half:].astype(BF16)
    stage[3] = to_left[:, :half].astype(BF16)
    arrivals = [send(2, rs_in.at[0, 1], 0), send(3, rs_in.at[1, 0], 1)]
    own[...] = on_chip(x)
    first[0].wait_recv()
    stage[4] = (to_right[:, :half] + half_in[0].astype(F32)).astype(BF16)
    arrivals.append(send(4, rs_in.at[0, 0], 0))
    first[1].wait_recv()
    stage[5] = (to_left[:, half:] + half_in[1].astype(F32)).astype(BF16)
    arrivals.append(send(5, rs_in.at[1, 1], 1))
    for copy in arrivals:
        copy.wait_recv()
    mine = pl.ds(pl.multiple_of(tp * rows, rows), rows)
    for i in range(2):
        cols = pl.ds(i * half, half)
        down_sum = own[:, cols] + rs_in[0, i].astype(F32) + rs_in[1, i].astype(F32)
        out_ref[:, cols] = (middle[mine, cols].astype(F32) + down_sum).astype(BF16)

    for copy in sends:
        copy.wait_send()
    wos.gone()
    ats.gone()
    for item in ITEMS:
        kv_prev(item).wait_send()
        kv_right(item, last).wait_send()
        kv_left(item, last).wait_send()

        @pl.when((y == 1) | (y == 2))
        def _():
            kv_relay_right(item).wait_send()
            kv_relay_left(item).wait_send()

    for i in range(3):
        d_copy(i).wait_send()

    def gone_z(way, r):
        z_copy(way, r).wait_send()
        for s in range(2):
            q_copy(way, r, s).wait_send()

    def gone_round(r, carry):
        gone_z(0, r)
        gone_z(1, r)
        return carry

    lax.fori_loop(0, hz - 1, gone_round, 0)
    gone_z(1, hz - 1)

    def gone_y(o, carry):
        y_copy(0, o).wait_send()
        y_copy(1, o).wait_send()
        y_across(o).wait_send()
        return carry

    lax.fori_loop(0, nz, gone_y, 0)


def local(n_sp, n_tp, residual, queries, keys, values, gate_cache, doc_ids, out_weight, mix_gain, gate_weight, up_weight, down_weight):
    tok, width = queries.shape
    d_model = out_weight.shape[1]
    rows = tok // n_tp
    wr, ff = gate_weight.shape
    heads = gate_cache.shape[1]
    both = jnp.concatenate(
        [gate_weight.reshape(wr, ff // 128, 1, 128), up_weight.reshape(wr, ff // 128, 1, 128)], axis=2
    ).reshape(wr, 2 * ff)
    early = (2 * ff) // 256 * 256 - 256
    late = jnp.concatenate([both[:, early:], down_weight.T], axis=1)
    aux = jnp.concatenate(
        [gate_cache.T, doc_ids.astype(F32)[None], jnp.zeros((8 - heads - 1, tok), F32)], axis=0
    )
    nz = n_sp // NY
    hz = nz // 2
    tile = 128
    half = d_model // 2
    vmem = pl.BlockSpec(memory_space=pltpu.VMEM)
    anywhere = pl.BlockSpec(memory_space=pl.ANY)
    dma = pltpu.SemaphoreType.DMA
    return pl.pallas_call(
        functools.partial(kernel, n_sp, n_tp),
        out_shape=jax.ShapeDtypeStruct((rows, d_model), BF16),
        in_specs=[vmem, anywhere, anywhere, anywhere, anywhere, anywhere, anywhere, anywhere, vmem],
        out_specs=vmem,
        scratch_shapes=[
            pltpu.VMEM(((REACH + 1) * tok, width), BF16),
            pltpu.VMEM(((REACH + 1) * tok, width), BF16),
            pltpu.VMEM((8, (REACH + 1) * tok), F32),
            pltpu.VMEM((n_sp, wr, early), BF16),
            pltpu.VMEM((n_sp, wr, 3 * ff - early), BF16),
            pltpu.VMEM((n_tp, width, d_model), BF16),
            pltpu.VMEM((tok, d_model), BF16),
            pltpu.VMEM((tile, REACH * tok + tile), F32),
            pltpu.VMEM((tok, 128), F32),
            pltpu.VMEM((tok, n_tp * width), BF16),
            pltpu.VMEM((n_tp // 2, 2, rows, d_model), BF16),
            pltpu.VMEM((n_tp // 2, rows, d_model), BF16),
            pltpu.VMEM((6, rows, half), BF16),
            pltpu.VMEM((rows, d_model), F32),
            pltpu.VMEM((2, rows, half), BF16),
            pltpu.VMEM((2, 2, rows, half), BF16),
            pltpu.VMEM((tok, d_model), BF16),
            pltpu.VMEM((tok, ff), BF16),
            pltpu.VMEM((tok, d_model), BF16),
            dma((7,)),
            dma((3, 5)),
            dma((3, 4)),
            dma((2, hz + 1)),
            dma((2, hz + 1)),
            dma((3, nz)),
            dma((3, nz)),
            dma((3,)),
            dma((3,)),
            dma((2, hz + 1, 2)),
            dma((2, hz + 1, 2)),
            dma((7,)),
            dma((7,)),
            dma((8, 4)),
            dma((8, 4)),
            dma((8, tok // tile)),
            dma((8, tok // tile)),
        ],
        compiler_params=pltpu.CompilerParams(
            collective_id=0, has_side_effects=True, vmem_limit_bytes=60 * 1024 * 1024
        ),
    )(queries, keys, values, aux, both[:, :early], late, out_weight, residual, mix_gain[None])


def solution(mesh):
    n_sp, n_tp = mesh.shape["sp"], mesh.shape["tp"]
    return jax.shard_map(
        functools.partial(local, n_sp, n_tp),
        mesh=mesh,
        in_specs=(
            P("sp", None), P("sp", "tp"), P("sp", "tp"), P("sp", "tp"), P("sp", "tp"), P("sp"),
            P("tp", None), P(), P("sp", "tp"), P("sp", "tp"), P("tp", "sp"),
        ),
        out_specs=P(("sp", "tp"), None),
        check_vma=False,
    )
```

```python
import functools
import math

import jax
import jax.numpy as jnp
from jax import lax
from jax.experimental import pallas as pl
from jax.experimental.pallas import tpu as pltpu
from jax.sharding import PartitionSpec as P

MESH = pl.DeviceIdType.MESH
EPSILON = 1e-06
NEGATIVE = -1e30
REACH = 4
NY = 4
LOG2E = math.log2(math.e)
F32 = jnp.float32
BF16 = jnp.bfloat16


def dot(a, b):
    return lax.dot_general(a, b, (((1,), (0,)), ((), ())), preferred_element_type=F32)


def dot_nt(a, b):
    return lax.dot_general(a, b, (((1,), (1,)), ((), ())), preferred_element_type=F32)


def kernel(
    n_sp, n_tp,
    q_ref, k_ref, v_ref, gates_ref, docs_ref, gate_ref, up_ref, down_ref, wo_ref, res_ref, gain_ref,
    out_ref,
    k_all, v_all, aux_all, gates, down, gu, qd, wo, res, bias, doc_col, att, part, pair,
    stage, own, half_in, rs_in, x_all, hidden, middle,
    loc, kv_s, kv_r, gz_s, gz_r, gy_s, gy_r, dy_s, dy_r, dz_s, dz_r, rs_s, rs_r, wo_s, wo_r, ag_s, ag_r,
):
    nz = n_sp // NY
    nx = n_tp // 2
    hz = nz // 2
    sp, tp = lax.axis_index("sp"), lax.axis_index("tp")
    z, y = sp // NY, sp % NY
    x, c = tp // 2, tp % 2
    tok, width = q_ref.shape
    heads = 4
    rows = tok // n_tp
    d_model = wo.shape[2]
    ff = hidden.shape[1]
    tile = 128
    n_tiles = tok // tile

    def at_sp(dz, dy):
        return ((z + dz + nz) % nz) * NY + (y + dy + NY) % NY

    def at_tp(dx, dc):
        return ((x + dx + nx) % nx) * 2 + (c + dc) % 2

    dev_z = ((at_sp(1, 0), tp), (at_sp(-1, 0), tp))
    dev_y = ((at_sp(0, 1), tp), (at_sp(0, -1), tp), (at_sp(0, 2), tp))
    dev_c = (sp, at_tp(0, 1))
    dev_x = ((sp, at_tp(1, 0)), (sp, at_tp(-1, 0)))

    def remote(src, dst, ssem, rsem, dev):
        return pltpu.make_async_remote_copy(
            src_ref=src, dst_ref=dst, send_sem=ssem, recv_sem=rsem, device_id=dev, device_id_type=MESH
        )

    last = REACH * tok
    extra = qd.shape[2] - ff
    pieces_of = [gu.at[sp, :, pl.ds(j * 128, 128)] for j in range(gu.shape[2] // 128)]
    pieces_of += [qd.at[sp, :, pl.ds(j * 128, 128)] for j in range(extra // 128)]
    local = [
        pltpu.make_async_copy(k_ref, k_all.at[pl.ds(last, tok)], loc.at[0]),
        pltpu.make_async_copy(v_ref, v_all.at[pl.ds(last, tok)], loc.at[1]),
        pltpu.make_async_copy(gates_ref, gates, loc.at[2]),
        pltpu.make_async_copy(down_ref, down, loc.at[3]),
        pltpu.make_async_copy(wo_ref, wo.at[tp], loc.at[4]),
        pltpu.make_async_copy(res_ref, res, loc.at[5]),
    ]
    shards = []
    for j, here in enumerate(pieces_of):
        ref = up_ref if j % 2 else gate_ref
        shards.append(pltpu.make_async_copy(ref.at[:, pl.ds(j // 2 * 128, 128)], here, loc.at[6 + j]))
    for copy in (local[2], local[3], *shards, local[0], local[1], local[4], local[5]):
        copy.start()

    barrier = pltpu.get_barrier_semaphore()
    peers = (*dev_z, *dev_y, dev_c, *dev_x)
    for peer in peers:
        pl.semaphore_signal(barrier, inc=1, device_id=peer, device_id_type=MESH)
    local[2].wait()
    aux_all[:, pl.ds(last, tok)] = jnp.zeros((8, tok), F32)
    aux_all[0:heads, pl.ds(last, tok)] = jnp.transpose(gates[...], (1, 0))
    aux_all[heads : heads + 1, pl.ds(last, tok)] = docs_ref[...].astype(F32)
    local[3].wait()
    turned = jnp.transpose(down[...].astype(F32), (1, 0)).astype(BF16)
    qd[sp, :, extra:] = turned
    pl.semaphore_wait(barrier, len(peers))

    def kv_slot(item, offset):
        if item == 2:
            return aux_all.at[:, pl.ds(pl.multiple_of(offset, 128), tok)]
        return (k_all, v_all)[item].at[pl.ds(pl.multiple_of(offset, 128), tok)]

    def kv_copy(item, kind, src, distance, dev):
        return remote(
            kv_slot(item, src), kv_slot(item, (REACH - distance) * tok),
            kv_s.at[item, kind], kv_r.at[item, distance - 1], dev,
        )

    def kv_prev(item):
        return kv_copy(item, 0, last, 4, dev_z[0])

    def kv_right(item, src):
        return kv_copy(item, 1, src, 1, dev_y[0])

    def kv_left(item, src):
        return kv_copy(item, 2, src, 3, dev_y[1])

    def kv_relay_right(item):
        return kv_copy(item, 3, (REACH - 1) * tok, 2, dev_y[0])

    def kv_relay_left(item):
        return kv_copy(item, 4, (REACH - 3) * tok, 2, dev_y[1])

    ITEMS = (2, 0, 1)

    def kv_own(item):
        if item < 2:
            local[item].wait()
        kv_prev(item).start()

        @pl.when(y < NY - 1)
        def _():
            kv_right(item, last).start()

        @pl.when(y == 0)
        def _():
            kv_left(item, last).start()

    def kv_turn(item):
        kv_prev(item).wait_recv()

        @pl.when(y == NY - 1)
        def _():
            kv_right(item, 0).start()

        @pl.when(y > 0)
        def _():
            kv_left(item, 0).start()

    def kv_relay(item):
        kv_right(item, last).wait_recv()

        @pl.when((y == 1) | (y == 2))
        def _():
            kv_relay_right(item).start()

        kv_left(item, last).wait_recv()

        @pl.when((y == 1) | (y == 2))
        def _():
            kv_relay_left(item).start()

    class Stream:
        def __init__(self, p, near, wide):
            self.p, self.near, self.wide = p, near, wide

        def z_move(self, way, r, step):
            block = self.near.at[at_sp(-r, 0) if way == 0 else at_sp(r, 0)]
            return remote(block, block, gz_s.at[self.p, way, r + step], gz_r.at[self.p, way, r + step], dev_z[way])

        def y_move(self, way, o, dy, lane):
            block, plane = self.near.at[at_sp(o, dy)], (o + nz) % nz
            return remote(block, block, gy_s.at[self.p, lane, plane], gy_r.at[self.p, lane, plane], dev_y[way])

        def y_arrival(self, way, o):
            return self.y_move(way, o, -1 if way == 0 else 1, way)

        def y_across(self, o):
            return self.y_move(0, o, 2, 2)

        def d_move(self, i, dy):
            block = self.wide.at[at_sp(0, dy)]
            return remote(block, block, dy_s.at[self.p, i], dy_r.at[self.p, i], dev_y[i])

        def q_move(self, way, r, s, step):
            plane = (z + (-r if way == 0 else r) + nz) % nz
            block = self.wide.at[pl.ds(plane * NY + s * (NY // 2), NY // 2)]
            return remote(
                block, block, dz_s.at[self.p, way, r + step, s], dz_r.at[self.p, way, r + step, s], dev_z[way]
            )

        def begin_wide(self):
            for i in range(3):
                self.d_move(i, 0).start()

        def begin_near_z(self):
            for way in range(2):
                self.z_move(way, 0, 1).start()

        def begin_near_y(self):
            for way in range(2):
                self.y_move(way, 0, 0, way).start()

        def begin_bundles(self):
            for i in range(3):
                self.d_move(i, (-1, 1, 2)[i]).wait_recv()
            for s in range(2):
                for way in range(2):
                    self.q_move(way, 0, s, 1).start()

        def along_z(self, r):
            fixed = isinstance(r, int)
            for way in range(2):
                count = hz - 1 + way
                if fixed and r > count:
                    continue
                self.z_move(way, r, 0).wait_recv()
                if not fixed or r < count:
                    self.z_move(way, r, 1).start()
                for side in range(2):
                    self.y_move(side, -r if way == 0 else r, 0, side).start()

        def bundles(self, r, s):
            fixed = isinstance(r, int)
            for way in range(2):
                count = hz - 1 + way
                if fixed and r > count:
                    continue
                self.q_move(way, r, s, 0).wait_recv()
                if not fixed or r < count:
                    self.q_move(way, r, s, 1).start()

        def along_y(self, r):
            fixed = isinstance(r, int)
            if not fixed or r < hz:
                self.y_arrival(0, -r).wait_recv()
                self.y_move(0, -r, -1, 2).start()

            def other():
                self.y_arrival(1, r).wait_recv()
                self.y_move(1, r, 1, 2).start()

            if not fixed:
                pl.when(r > 0)(other)
            elif r > 0:
                other()

        def arrive(self, r):
            if r < hz:
                self.y_arrival(1, -r).wait_recv()
                self.y_across(-r).wait_recv()
            if r > 0:
                self.y_arrival(0, r).wait_recv()
                self.y_across(r).wait_recv()

        def pieces(self, k):
            ahead = k + AHEAD
            return [
                functools.partial(self.along_z, ahead),
                functools.partial(self.bundles, k, 0),
                functools.partial(self.along_y, ahead - 1),
                functools.partial(self.bundles, k, 1),
            ]

        def gone(self):
            for i in range(3):
                self.d_move(i, 0).wait_send()

            def ring(way, r):
                self.z_move(way, r, 1).wait_send()
                for s in range(2):
                    self.q_move(way, r, s, 1).wait_send()

            def both(r, carry):
                ring(0, r)
                ring(1, r)
                return carry

            lax.fori_loop(0, hz - 1, both, 0)
            ring(1, hz - 1)

            def side(o, carry):
                for lane in range(3):
                    self.y_move(0, o, 0, lane).wait_send()
                return carry

            lax.fori_loop(0, nz, side, 0)

    AHEAD = 1
    stream = Stream(0, gu, qd)
    queue = []
    for k in range(1, hz + 1):
        steps = stream.pieces(k)
        keep = (k + AHEAD <= hz, True, k + AHEAD - 1 <= hz, True)
        queue += [step for step, wanted in zip(steps, keep) if wanted]

    def serve(count):
        for _ in range(min(count, len(queue))):
            queue.pop(0)()

    class Gather:
        def __init__(self, view, send, recv, count):
            self.view, self.send, self.recv, self.count = view, send, recv, count

        def copy(self, kind, slot, j):
            ref = self.view(slot, j, {2: 0, 3: 1}.get(kind))
            dev = dev_c if kind >= 4 else dev_x[kind % 2]
            return remote(ref, ref, self.send.at[kind, j], self.recv.at[kind, j], dev)

        def begin(self, j):
            for kind in (0, 1, 4):
                self.copy(kind, tp, j).start()

        def near(self, j):
            for way in range(2):
                slot = at_tp(2 * way - 1, 0)
                self.copy(way, slot, j).wait_recv()
                self.copy(2 + way, slot, j).start()
                self.copy(5 + way, slot, j).start()

        def far(self, j):
            slot = at_tp(2, 0)
            self.copy(2, slot, j).wait_recv()
            self.copy(3, slot, j).wait_recv()
            self.copy(7, slot, j).start()

        def done(self, j):
            for kind, dx in ((4, 0), (5, -1), (6, 1), (7, 2)):
                self.copy(kind, at_tp(dx, 1), j).wait_recv()

        def gone(self):
            for kind in range(8):
                for j in range(self.count):
                    self.copy(kind, tp, j).wait_send()

    def wo_view(slot, j, part_of):
        size = width // 4
        if part_of is None:
            return wo.at[slot, pl.ds(j * size, size)]
        return wo.at[slot, pl.ds(j * size + part_of * (size // 2), size // 2)]

    def att_view(slot, j, part_of):
        cols = pl.ds(pl.multiple_of(slot * width, 128), width)
        if part_of is None:
            return att.at[pl.ds(pl.multiple_of(j * tile, tile), tile), cols]
        return att.at[pl.ds(pl.multiple_of(j * tile + part_of * (tile // 2), tile // 2), tile // 2), cols]

    wos = Gather(wo_view, wo_s, wo_r, 4)
    ats = Gather(att_view, ag_s, ag_r, n_tiles)

    for copy in shards:
        copy.wait()
    stream.begin_near_z()
    stream.begin_wide()
    for item in ITEMS:
        kv_own(item)
    stream.begin_near_y()
    local[4].wait()
    for j in range(4):
        wos.begin(j)
    stream.along_z(1)
    stream.begin_bundles()
    kv_turn(2)
    kv_turn(0)
    wos.near(0)
    kv_turn(1)
    stream.along_y(0)
    kv_relay(2)
    kv_relay(0)
    wos.near(1)
    serve(2)
    kv_relay(1)
    serve(2)
    wos.near(2)
    serve(4)
    wos.near(3)
    for item in ITEMS:
        kv_relay_right(item).wait_recv()

    window = REACH * tok + tile
    lanes = lax.broadcasted_iota(jnp.int32, (1, width), 1) // (width // heads)
    scale = (width // heads) ** -0.5 * LOG2E
    own_docs = jnp.transpose(aux_all[:, pl.ds(last, tok)], (1, 0))
    origin = own_docs[0:1, 0:heads]
    doc_col[...] = jnp.broadcast_to(own_docs[:, heads : heads + 1], doc_col.shape)
    own_cols = pl.ds(pl.multiple_of(tp * width, 128), width)

    def attend(i, carry):
        start = pl.multiple_of(i * tile, tile)
        doc_row = aux_all[heads : heads + 1, pl.ds(start, window)]
        doc_here = doc_col[pl.ds(start, tile), 0:1]
        gap = lax.broadcasted_iota(jnp.int32, (tile, window), 1) - lax.broadcasted_iota(jnp.int32, (tile, window), 0)
        bias[...] = jnp.where((doc_row == doc_here) & (gap <= REACH * tok), 0.0, NEGATIVE)
        queries = q_ref[pl.ds(start, tile), :]
        keys = k_all[pl.ds(start, window), :]
        values = v_all[pl.ds(start, window), :]
        total = jnp.zeros((tile, width), F32)
        service = stream.pieces(i + 3)
        for h in range(heads):
            masked = jnp.where(lanes == h, queries, jnp.zeros_like(queries))
            gates = (origin[:, h : h + 1] - aux_all[h : h + 1, pl.ds(start, window)]) * LOG2E
            scores = dot_nt(masked, keys) * scale + gates + bias[...]
            peak = jnp.max(scores, axis=-1, keepdims=True)
            weights = jnp.exp2(scores - peak)
            norm = jnp.sum(weights, axis=-1, keepdims=True)
            mixed = dot(weights.astype(BF16), values)
            total = jnp.where(lanes == h, mixed / norm, total)
            if h == heads - 1:
                att[pl.ds(start, tile), own_cols] = total.astype(BF16)
                ats.begin(i)

            @pl.when(i < n_tiles - 1)
            def _():
                service[h]()

        wos.far(i)

        @pl.when(i >= 1)
        def _():
            ats.near(i - 1)

        return carry

    lax.fori_loop(0, n_tiles, attend, 0)
    del queue[: 4 * (n_tiles - 1)]

    n_tile = 256

    def project(i):
        block = pl.ds(i * tile, tile)

        def columns(n, carry):
            cols = pl.ds(pl.multiple_of(n * n_tile, n_tile), n_tile)
            product = dot(att[block, :], wo[:, :, cols].reshape(n_tp * width, n_tile))
            middle[block, cols] = (res[block, cols].astype(F32) + product).astype(BF16)
            return carry

        lax.fori_loop(0, d_model // n_tile, columns, 0)
        wide = middle[block, :].astype(F32)
        factor = lax.rsqrt(jnp.mean(wide * wide, axis=-1, keepdims=True) + EPSILON)
        x_all[block, :] = (wide * factor * gain_ref[...]).astype(BF16)

    ats.far(0)
    wos.far(3)
    ats.near(2)
    serve(2)
    for j in range(4):
        wos.done(j)
    ats.done(0)
    local[5].wait()
    project(0)
    serve(3)
    ats.far(1)
    ats.far(2)
    ats.done(1)
    project(1)
    serve(3)
    ats.done(2)
    project(2)
    serve(len(queue))
    for r in range(hz + 1):
        stream.arrive(r)

    def activate(both, n):
        gate, up = both[:, :128], both[:, 128:]
        hidden[:, pl.ds(pl.multiple_of(n * 128, 128), 128)] = (gate / (1.0 + jnp.exp(-gate)) * up).astype(BF16)

    early = gu.shape[2] // 256

    def expand(n, carry):
        cols = pl.ds(pl.multiple_of(n * 256, 256), 256)
        activate(dot(x_all[...], gu[:, :, cols].reshape(d_model, 256)), n)
        return carry

    lax.fori_loop(0, early, expand, 0)
    mixed = jnp.concatenate(
        [gu[:, :, early * 256 :].reshape(d_model, 128), qd[:, :, :extra].reshape(d_model, 128)], axis=1
    )
    activate(dot(x_all[...], mixed), early)

    order = [0]
    for r in range(1, hz):
        order += [r, -r]
    order.append(hz)
    groups = [order[i : i + 4] for i in range(0, nz, 4)]
    span = d_model // nz
    sends = []
    half = 2 * span
    opposite, right, left = (x + 2) % nx, (x + 1) % nx, (x + nx - 1) % nx

    def plane_of(o):
        return (z + o + nz) % nz

    def on_chip(g, there):
        return part[g, there, c].astype(F32) + pair[g, there].astype(F32)

    def swap_of(g):
        return remote(part.at[g, :, 1 - c], pair.at[g], rs_s.at[g, 0], rs_r.at[g, 0], dev_c)

    def send_of(g, i):
        dst = (
            half_in.at[g, 0], half_in.at[g, 1], rs_in.at[g, 0, 1], rs_in.at[g, 1, 0], rs_in.at[g, 0, 0], rs_in.at[g, 1, 1]
        )[i]
        return remote(stage.at[g, i], dst, rs_s.at[g, i + 1], rs_r.at[g, i + 1], dev_x[i % 2])

    def contract(g):
        for i in range(2):
            planes = [pl.ds(plane_of(o) * NY, NY) for o in groups[g][2 * i : 2 * i + 2]]
            block = jnp.concatenate([qd[p, :, extra:].reshape(span, ff) for p in planes], axis=0)
            part[g, :, :, :, i * half : (i + 1) * half] = dot_nt(hidden[...], block).astype(BF16).reshape(nx, 2, rows, half)
        swap_of(g).start()

    def outward(g):
        swap_of(g).wait_recv()
        total = on_chip(g, opposite).astype(BF16)
        stage[g, 0] = total[:, :half]
        stage[g, 1] = total[:, half:]
        send_of(g, 0).start()
        send_of(g, 1).start()
        stage[g, 2] = on_chip(g, right)[:, half:].astype(BF16)
        stage[g, 3] = on_chip(g, left)[:, :half].astype(BF16)
        send_of(g, 2).start()
        send_of(g, 3).start()

    def onward(g):
        send_of(g, 0).wait_recv()
        stage[g, 4] = (on_chip(g, right)[:, :half] + half_in[g, 0].astype(F32)).astype(BF16)
        send_of(g, 4).start()
        send_of(g, 1).wait_recv()
        stage[g, 5] = (on_chip(g, left)[:, half:] + half_in[g, 1].astype(F32)).astype(BF16)
        send_of(g, 5).start()

    mine = pl.ds(pl.multiple_of(tp * rows, rows), rows)

    def finish(g):
        own[...] = on_chip(g, x)
        for i in range(2, 6):
            send_of(g, i).wait_recv()
        for j, o in enumerate(groups[g]):
            i, at = j // 2, (j % 2) * span
            cols = pl.ds(pl.multiple_of(plane_of(o) * span, span), span)
            down_sum = (
                own[:, j * span : (j + 1) * span]
                + rs_in[g, 0, i, :, at : at + span].astype(F32)
                + rs_in[g, 1, i, :, at : at + span].astype(F32)
            )
            out_ref[:, cols] = (middle[mine, cols].astype(F32) + down_sum).astype(BF16)

    steps = (contract, outward, onward, finish)
    for t in range(len(groups) + len(steps) - 1):
        for k, step in enumerate(steps):
            if 0 <= t - k < len(groups):
                step(t - k)

    for g in range(len(groups)):
        swap_of(g).wait_send()
        for i in range(6):
            send_of(g, i).wait_send()
    wos.gone()
    ats.gone()
    for item in ITEMS:
        kv_prev(item).wait_send()
        kv_right(item, last).wait_send()
        kv_left(item, last).wait_send()

        @pl.when((y == 1) | (y == 2))
        def _():
            kv_relay_right(item).wait_send()
            kv_relay_left(item).wait_send()

    stream.gone()


def local(n_sp, n_tp, residual, queries, keys, values, gate_cache, doc_ids, out_weight, mix_gain, gate_weight, up_weight, down_weight):
    tok, width = queries.shape
    d_model = out_weight.shape[1]
    rows = tok // n_tp
    wr, ff = gate_weight.shape
    heads = gate_cache.shape[1]
    nz = n_sp // NY
    hz = nz // 2
    tile = 128
    early = 9 * 128
    span = d_model // nz
    n_groups = nz // 4
    vmem = pl.BlockSpec(memory_space=pltpu.VMEM)
    anywhere = pl.BlockSpec(memory_space=pl.ANY)
    dma = pltpu.SemaphoreType.DMA
    return pl.pallas_call(
        functools.partial(kernel, n_sp, n_tp),
        out_shape=jax.ShapeDtypeStruct((rows, d_model), BF16),
        in_specs=[vmem, *[anywhere] * 3, vmem, *[anywhere] * 5, vmem],
        out_specs=vmem,
        scratch_shapes=[
            pltpu.VMEM(((REACH + 1) * tok, width), BF16),
            pltpu.VMEM(((REACH + 1) * tok, width), BF16),
            pltpu.VMEM((8, (REACH + 1) * tok), F32),
            pltpu.VMEM((tok, heads), F32),
            pltpu.VMEM((ff, wr), BF16),
            pltpu.VMEM((n_sp, wr, early), BF16),
            pltpu.VMEM((n_sp, wr, 3 * ff - early), BF16),
            pltpu.VMEM((n_tp, width, d_model), BF16),
            pltpu.VMEM((tok, d_model), BF16),
            pltpu.VMEM((tile, REACH * tok + tile), F32),
            pltpu.VMEM((tok, 128), F32),
            pltpu.VMEM((tok, n_tp * width), BF16),
            pltpu.VMEM((n_groups, n_tp // 2, 2, rows, 4 * span), BF16),
            pltpu.VMEM((n_groups, n_tp // 2, rows, 4 * span), BF16),
            pltpu.VMEM((n_groups, 6, rows, 2 * span), BF16),
            pltpu.VMEM((rows, 4 * span), F32),
            pltpu.VMEM((n_groups, 2, rows, 2 * span), BF16),
            pltpu.VMEM((n_groups, 2, 2, rows, 2 * span), BF16),
            pltpu.VMEM((tok, d_model), BF16),
            pltpu.VMEM((tok, ff), BF16),
            pltpu.VMEM((tok, d_model), BF16),
            dma((6 + ff // 64,)),
            dma((3, 5)),
            dma((3, 4)),
            dma((1, 2, hz + 1)),
            dma((1, 2, hz + 1)),
            dma((1, 3, nz)),
            dma((1, 3, nz)),
            dma((1, 3)),
            dma((1, 3)),
            dma((1, 2, hz + 1, 2)),
            dma((1, 2, hz + 1, 2)),
            dma((n_groups, 7)),
            dma((n_groups, 7)),
            dma((8, 4)),
            dma((8, 4)),
            dma((8, tok // tile)),
            dma((8, tok // tile)),
        ],
        compiler_params=pltpu.CompilerParams(
            collective_id=0, has_side_effects=True, vmem_limit_bytes=60 * 1024 * 1024
        ),
    )(
        queries, keys, values, gate_cache, doc_ids[None], gate_weight, up_weight, down_weight, out_weight, residual, mix_gain[None]
    )


def solution(mesh):
    n_sp, n_tp = mesh.shape["sp"], mesh.shape["tp"]
    return jax.shard_map(
        functools.partial(local, n_sp, n_tp),
        mesh=mesh,
        in_specs=(
            P("sp", None), P("sp", "tp"), P("sp", "tp"), P("sp", "tp"), P("sp", "tp"), P("sp"),
            P("tp", None), P(), P("sp", "tp"), P("sp", "tp"), P("tp", "sp"),
        ),
        out_specs=P(("sp", "tp"), None),
        check_vma=False,
    )
```

```python
import functools
import math

import jax
import jax.numpy as jnp
from jax import lax
from jax.experimental import pallas as pl
from jax.experimental.pallas import tpu as pltpu
from jax.sharding import PartitionSpec as P

MESH = pl.DeviceIdType.MESH
EPSILON = 1e-06
NEGATIVE = -1e30
REACH = 4
NY = 4
LOG2E = math.log2(math.e)
F32 = jnp.float32
BF16 = jnp.bfloat16


def dot(a, b):
    return lax.dot_general(a, b, (((1,), (0,)), ((), ())), preferred_element_type=F32)


def dot_nt(a, b):
    return lax.dot_general(a, b, (((1,), (1,)), ((), ())), preferred_element_type=F32)


def kernel(
    n_sp, n_tp,
    q_ref, k_ref, v_ref, gates_ref, docs_ref, gate_ref, up_ref, down_ref, wo_ref, res_ref, gain_ref,
    out_ref,
    k_all, v_all, aux_all, gates, down, gu, qd, wo, res, bias, doc_col, att, part, pair,
    stage, own, half_in, rs_in, x_all, hidden, middle,
    loc, kv_s, kv_r, gz_s, gz_r, gy_s, gy_r, dy_s, dy_r, dz_s, dz_r, rs_s, rs_r, wo_s, wo_r, ag_s, ag_r,
):
    nz = n_sp // NY
    nx = n_tp // 2
    hz = nz // 2
    sp, tp = lax.axis_index("sp"), lax.axis_index("tp")
    z, y = sp // NY, sp % NY
    x, c = tp // 2, tp % 2
    tok, width = q_ref.shape
    heads = 4
    rows = tok // n_tp
    d_model = wo.shape[2]
    ff = hidden.shape[1]
    tile = 128
    n_tiles = tok // tile

    def at_sp(dz, dy):
        return ((z + dz + nz) % nz) * NY + (y + dy + NY) % NY

    def at_tp(dx, dc):
        return ((x + dx + nx) % nx) * 2 + (c + dc) % 2

    dev_z = ((at_sp(1, 0), tp), (at_sp(-1, 0), tp))
    dev_y = ((at_sp(0, 1), tp), (at_sp(0, -1), tp), (at_sp(0, 2), tp))
    dev_c = (sp, at_tp(0, 1))
    dev_x = ((sp, at_tp(1, 0)), (sp, at_tp(-1, 0)))

    def remote(src, dst, ssem, rsem, dev):
        return pltpu.make_async_remote_copy(
            src_ref=src, dst_ref=dst, send_sem=ssem, recv_sem=rsem, device_id=dev, device_id_type=MESH
        )

    last = REACH * tok
    extra = qd.shape[2] - ff
    pieces_of = [gu.at[sp, :, pl.ds(j * 128, 128)] for j in range(gu.shape[2] // 128)]
    pieces_of += [qd.at[sp, :, pl.ds(j * 128, 128)] for j in range(extra // 128)]
    local = [
        pltpu.make_async_copy(k_ref, k_all.at[pl.ds(last, tok)], loc.at[0]),
        pltpu.make_async_copy(v_ref, v_all.at[pl.ds(last, tok)], loc.at[1]),
        pltpu.make_async_copy(gates_ref, gates, loc.at[2]),
        pltpu.make_async_copy(down_ref, down, loc.at[3]),
        pltpu.make_async_copy(wo_ref, wo.at[tp], loc.at[4]),
        pltpu.make_async_copy(res_ref, res, loc.at[5]),
    ]
    shards = []
    for j, here in enumerate(pieces_of):
        ref = up_ref if j % 2 else gate_ref
        shards.append(pltpu.make_async_copy(ref.at[:, pl.ds(j // 2 * 128, 128)], here, loc.at[6 + j]))
    for copy in (local[2], local[3], *shards, local[0], local[1], local[4], local[5]):
        copy.start()

    barrier = pltpu.get_barrier_semaphore()
    peers = (*dev_z, *dev_y, dev_c, *dev_x)
    for peer in peers:
        pl.semaphore_signal(barrier, inc=1, device_id=peer, device_id_type=MESH)
    local[2].wait()
    aux_all[:, pl.ds(last, tok)] = jnp.zeros((8, tok), F32)
    aux_all[0:heads, pl.ds(last, tok)] = jnp.transpose(gates[...], (1, 0))
    aux_all[heads : heads + 1, pl.ds(last, tok)] = docs_ref[...].astype(F32)
    local[3].wait()
    turned = jnp.transpose(down[...].astype(F32), (1, 0)).astype(BF16)
    qd[sp, :, extra:] = turned
    pl.semaphore_wait(barrier, len(peers))

    def kv_slot(item, offset):
        if item == 2:
            return aux_all.at[:, pl.ds(pl.multiple_of(offset, 128), tok)]
        return (k_all, v_all)[item].at[pl.ds(pl.multiple_of(offset, 128), tok)]

    def kv_copy(item, kind, src, distance, dev):
        return remote(
            kv_slot(item, src), kv_slot(item, (REACH - distance) * tok),
            kv_s.at[item, kind], kv_r.at[item, distance - 1], dev,
        )

    def kv_prev(item):
        return kv_copy(item, 0, last, 4, dev_z[0])

    def kv_right(item, src):
        return kv_copy(item, 1, src, 1, dev_y[0])

    def kv_left(item, src):
        return kv_copy(item, 2, src, 3, dev_y[1])

    def kv_relay_right(item):
        return kv_copy(item, 3, (REACH - 1) * tok, 2, dev_y[0])

    def kv_relay_left(item):
        return kv_copy(item, 4, (REACH - 3) * tok, 2, dev_y[1])

    ITEMS = (2, 0, 1)

    def kv_own(item):
        if item < 2:
            local[item].wait()
        kv_prev(item).start()

        @pl.when(y < NY - 1)
        def _():
            kv_right(item, last).start()

        @pl.when(y == 0)
        def _():
            kv_left(item, last).start()

    def kv_turn(item):
        kv_prev(item).wait_recv()

        @pl.when(y == NY - 1)
        def _():
            kv_right(item, 0).start()

        @pl.when(y > 0)
        def _():
            kv_left(item, 0).start()

    def kv_relay(item):
        kv_right(item, last).wait_recv()

        @pl.when((y == 1) | (y == 2))
        def _():
            kv_relay_right(item).start()

        kv_left(item, last).wait_recv()

        @pl.when((y == 1) | (y == 2))
        def _():
            kv_relay_left(item).start()

    class Stream:
        def __init__(self, p, near, wide):
            self.p, self.near, self.wide = p, near, wide

        def z_move(self, way, r, step):
            block = self.near.at[at_sp(-r, 0) if way == 0 else at_sp(r, 0)]
            return remote(block, block, gz_s.at[self.p, way, r + step], gz_r.at[self.p, way, r + step], dev_z[way])

        def y_move(self, way, o, dy, lane):
            block, plane = self.near.at[at_sp(o, dy)], (o + nz) % nz
            return remote(block, block, gy_s.at[self.p, lane, plane], gy_r.at[self.p, lane, plane], dev_y[way])

        def y_arrival(self, way, o):
            return self.y_move(way, o, -1 if way == 0 else 1, way)

        def y_across(self, o):
            return self.y_move(0, o, 2, 2)

        def d_move(self, i, dy):
            block = self.wide.at[at_sp(0, dy)]
            return remote(block, block, dy_s.at[self.p, i], dy_r.at[self.p, i], dev_y[i])

        def q_move(self, way, r, s, step):
            plane = (z + (-r if way == 0 else r) + nz) % nz
            block = self.wide.at[pl.ds(plane * NY + s * (NY // 2), NY // 2)]
            return remote(
                block, block, dz_s.at[self.p, way, r + step, s], dz_r.at[self.p, way, r + step, s], dev_z[way]
            )

        def begin_wide(self):
            for i in range(3):
                self.d_move(i, 0).start()

        def begin_near_z(self):
            for way in range(2):
                self.z_move(way, 0, 1).start()

        def begin_near_y(self):
            for way in range(2):
                self.y_move(way, 0, 0, way).start()

        def begin_bundles(self):
            for i in range(3):
                self.d_move(i, (-1, 1, 2)[i]).wait_recv()
            for s in range(2):
                for way in range(2):
                    self.q_move(way, 0, s, 1).start()

        def ways(self, k):
            return [(way, k + way) for way in range(2) if not (isinstance(k, int) and k == 0 and way == 0)]

        def along_z(self, k):
            for way, r in self.ways(k):
                self.z_move(way, r, 0).wait_recv()
                if not isinstance(k, int) or k < hz - 1:
                    self.z_move(way, r, 1).start()
                for side in range(2):
                    self.y_move(side, -r if way == 0 else r, 0, side).start()

        def bundles(self, k, s):
            for way, r in self.ways(k):
                self.q_move(way, r, s, 0).wait_recv()
                if not isinstance(k, int) or k < hz - 1:
                    self.q_move(way, r, s, 1).start()

        def along_y(self, k):
            self.y_arrival(0, -k).wait_recv()
            self.y_move(0, -k, -1, 2).start()
            self.y_arrival(1, k + 1).wait_recv()
            self.y_move(1, k + 1, 1, 2).start()

        def arrive(self, r):
            if r < hz:
                self.y_arrival(1, -r).wait_recv()
                self.y_across(-r).wait_recv()
            if r > 0:
                self.y_arrival(0, r).wait_recv()
                self.y_across(r).wait_recv()

        def pieces(self, k):
            return [
                functools.partial(self.along_z, k + 1),
                functools.partial(self.bundles, k, 0),
                functools.partial(self.along_y, k),
                functools.partial(self.bundles, k, 1),
            ]

        def gone(self):
            for i in range(3):
                self.d_move(i, 0).wait_send()

            def ring(way, r):
                self.z_move(way, r, 1).wait_send()
                for s in range(2):
                    self.q_move(way, r, s, 1).wait_send()

            def both(r, carry):
                ring(0, r)
                ring(1, r)
                return carry

            lax.fori_loop(0, hz - 1, both, 0)
            ring(1, hz - 1)

            def side(o, carry):
                for lane in range(3):
                    self.y_move(0, o, 0, lane).wait_send()
                return carry

            lax.fori_loop(0, nz, side, 0)

    stream = Stream(0, gu, qd)
    queue = []
    for k in range(1, hz):
        steps = stream.pieces(k)
        queue += steps if k + 1 < hz else steps[1:]

    def serve(count):
        for _ in range(min(count, len(queue))):
            queue.pop(0)()

    class Gather:
        def __init__(self, view, send, recv, count):
            self.view, self.send, self.recv, self.count = view, send, recv, count

        def copy(self, kind, slot, j):
            ref = self.view(slot, j, {2: 0, 3: 1}.get(kind))
            dev = dev_c if kind >= 4 else dev_x[kind % 2]
            return remote(ref, ref, self.send.at[kind, j], self.recv.at[kind, j], dev)

        def begin(self, j):
            for kind in (0, 1, 4):
                self.copy(kind, tp, j).start()

        def near(self, j):
            for way in range(2):
                slot = at_tp(2 * way - 1, 0)
                self.copy(way, slot, j).wait_recv()
                self.copy(2 + way, slot, j).start()
                self.copy(5 + way, slot, j).start()

        def far(self, j):
            slot = at_tp(2, 0)
            self.copy(2, slot, j).wait_recv()
            self.copy(3, slot, j).wait_recv()
            self.copy(7, slot, j).start()

        def done(self, j):
            for kind, dx in ((4, 0), (5, -1), (6, 1), (7, 2)):
                self.copy(kind, at_tp(dx, 1), j).wait_recv()

        def gone(self):
            for kind in range(8):
                for j in range(self.count):
                    self.copy(kind, tp, j).wait_send()

    def wo_view(slot, j, part_of):
        size = width // 4
        if part_of is None:
            return wo.at[slot, pl.ds(j * size, size)]
        return wo.at[slot, pl.ds(j * size + part_of * (size // 2), size // 2)]

    def att_view(slot, j, part_of):
        cols = pl.ds(pl.multiple_of(slot * width, 128), width)
        if part_of is None:
            return att.at[pl.ds(pl.multiple_of(j * tile, tile), tile), cols]
        return att.at[pl.ds(pl.multiple_of(j * tile + part_of * (tile // 2), tile // 2), tile // 2), cols]

    wos = Gather(wo_view, wo_s, wo_r, 4)
    ats = Gather(att_view, ag_s, ag_r, n_tiles)

    for copy in shards:
        copy.wait()
    stream.begin_near_z()
    stream.begin_wide()
    for item in ITEMS:
        kv_own(item)
    stream.begin_near_y()
    local[4].wait()
    for j in range(4):
        wos.begin(j)
    stream.along_z(0)
    stream.begin_bundles()
    kv_turn(2)
    kv_turn(0)
    wos.near(0)
    stream.bundles(0, 0)
    kv_turn(1)
    stream.along_z(1)
    stream.bundles(0, 1)
    stream.along_y(0)
    kv_relay(2)
    kv_relay(0)
    wos.near(1)
    serve(2)
    kv_relay(1)
    serve(2)
    wos.near(2)
    serve(4)
    wos.near(3)
    for item in ITEMS:
        kv_relay_right(item).wait_recv()

    window = REACH * tok + tile
    lanes = lax.broadcasted_iota(jnp.int32, (1, width), 1) // (width // heads)
    scale = (width // heads) ** -0.5 * LOG2E
    own_docs = jnp.transpose(aux_all[:, pl.ds(last, tok)], (1, 0))
    origin = own_docs[0:1, 0:heads]
    doc_col[...] = jnp.broadcast_to(own_docs[:, heads : heads + 1], doc_col.shape)
    own_cols = pl.ds(pl.multiple_of(tp * width, 128), width)

    def attend(i, carry):
        start = pl.multiple_of(i * tile, tile)
        doc_row = aux_all[heads : heads + 1, pl.ds(start, window)]
        doc_here = doc_col[pl.ds(start, tile), 0:1]
        gap = lax.broadcasted_iota(jnp.int32, (tile, window), 1) - lax.broadcasted_iota(jnp.int32, (tile, window), 0)
        bias[...] = jnp.where((doc_row == doc_here) & (gap <= REACH * tok), 0.0, NEGATIVE)
        queries = q_ref[pl.ds(start, tile), :]
        keys = k_all[pl.ds(start, window), :]
        values = v_all[pl.ds(start, window), :]
        total = jnp.zeros((tile, width), F32)
        service = stream.pieces(i + 3)
        for h in range(heads):
            masked = jnp.where(lanes == h, queries, jnp.zeros_like(queries))
            gates = (origin[:, h : h + 1] - aux_all[h : h + 1, pl.ds(start, window)]) * LOG2E
            scores = dot_nt(masked, keys) * scale + gates + bias[...]
            peak = jnp.max(scores, axis=-1, keepdims=True)
            weights = jnp.exp2(scores - peak)
            norm = jnp.sum(weights, axis=-1, keepdims=True)
            mixed = dot(weights.astype(BF16), values)
            total = jnp.where(lanes == h, mixed / norm, total)
            if h == heads - 1:
                att[pl.ds(start, tile), own_cols] = total.astype(BF16)
                ats.begin(i)

            service[h]()

        wos.far(i)

        @pl.when(i >= 1)
        def _():
            ats.near(i - 1)

        return carry

    lax.fori_loop(0, n_tiles, attend, 0)
    del queue[: 4 * n_tiles]

    n_tile = 256

    def project(i):
        block = pl.ds(i * tile, tile)

        def columns(n, carry):
            cols = pl.ds(pl.multiple_of(n * n_tile, n_tile), n_tile)
            product = dot(att[block, :], wo[:, :, cols].reshape(n_tp * width, n_tile))
            middle[block, cols] = (res[block, cols].astype(F32) + product).astype(BF16)
            return carry

        cuts = d_model // n_tile // 2
        lax.fori_loop(0, cuts, columns, 0)
        serve(1)
        lax.fori_loop(cuts, 2 * cuts, columns, 0)
        wide = middle[block, :].astype(F32)
        factor = lax.rsqrt(jnp.mean(wide * wide, axis=-1, keepdims=True) + EPSILON)
        x_all[block, :] = (wide * factor * gain_ref[...]).astype(BF16)

    ats.far(0)
    wos.far(3)
    ats.near(2)
    serve(3)
    for j in range(4):
        wos.done(j)
    ats.done(0)
    local[5].wait()
    project(0)
    serve(1)
    ats.far(1)
    ats.far(2)
    ats.done(1)
    project(1)
    serve(1)
    ats.done(2)
    project(2)
    serve(len(queue))
    for r in range(hz + 1):
        stream.arrive(r)

    def activate(both, n):
        gate, up = both[:, :128], both[:, 128:]
        hidden[:, pl.ds(pl.multiple_of(n * 128, 128), 128)] = (gate / (1.0 + jnp.exp(-gate)) * up).astype(BF16)

    early = gu.shape[2] // 256

    def expand(n, carry):
        cols = pl.ds(pl.multiple_of(n * 256, 256), 256)
        activate(dot(x_all[...], gu[:, :, cols].reshape(d_model, 256)), n)
        return carry

    lax.fori_loop(0, early, expand, 0)
    mixed = jnp.concatenate(
        [gu[:, :, early * 256 :].reshape(d_model, 128), qd[:, :, :extra].reshape(d_model, 128)], axis=1
    )
    activate(dot(x_all[...], mixed), early)

    order = [0]
    for r in range(1, hz):
        order += [r, -r]
    order.append(hz)
    groups = [order[i : i + 4] for i in range(0, nz, 4)]
    span = d_model // nz
    sends = []
    half = 2 * span
    opposite, right, left = (x + 2) % nx, (x + 1) % nx, (x + nx - 1) % nx

    def plane_of(o):
        return (z + o + nz) % nz

    def on_chip(g, there):
        return part[g, there, c].astype(F32) + pair[g, there].astype(F32)

    def swap_of(g):
        return remote(part.at[g, :, 1 - c], pair.at[g], rs_s.at[g, 0], rs_r.at[g, 0], dev_c)

    def send_of(g, i):
        dst = (
            half_in.at[g, 0], half_in.at[g, 1], rs_in.at[g, 0, 1], rs_in.at[g, 1, 0], rs_in.at[g, 0, 0], rs_in.at[g, 1, 1]
        )[i]
        return remote(stage.at[g, i], dst, rs_s.at[g, i + 1], rs_r.at[g, i + 1], dev_x[i % 2])

    def contract(g):
        for i in range(2):
            planes = [pl.ds(plane_of(o) * NY, NY) for o in groups[g][2 * i : 2 * i + 2]]
            block = jnp.concatenate([qd[p, :, extra:].reshape(span, ff) for p in planes], axis=0)
            part[g, :, :, :, i * half : (i + 1) * half] = dot_nt(hidden[...], block).astype(BF16).reshape(nx, 2, rows, half)
        swap_of(g).start()

    def outward(g):
        swap_of(g).wait_recv()
        total = on_chip(g, opposite).astype(BF16)
        stage[g, 0] = total[:, :half]
        stage[g, 1] = total[:, half:]
        send_of(g, 0).start()
        send_of(g, 1).start()
        stage[g, 2] = on_chip(g, right)[:, half:].astype(BF16)
        stage[g, 3] = on_chip(g, left)[:, :half].astype(BF16)
        send_of(g, 2).start()
        send_of(g, 3).start()

    def onward(g):
        send_of(g, 0).wait_recv()
        stage[g, 4] = (on_chip(g, right)[:, :half] + half_in[g, 0].astype(F32)).astype(BF16)
        send_of(g, 4).start()
        send_of(g, 1).wait_recv()
        stage[g, 5] = (on_chip(g, left)[:, half:] + half_in[g, 1].astype(F32)).astype(BF16)
        send_of(g, 5).start()

    mine = pl.ds(pl.multiple_of(tp * rows, rows), rows)

    def finish(g):
        own[...] = on_chip(g, x)
        for i in range(2, 6):
            send_of(g, i).wait_recv()
        for j, o in enumerate(groups[g]):
            i, at = j // 2, (j % 2) * span
            cols = pl.ds(pl.multiple_of(plane_of(o) * span, span), span)
            down_sum = (
                own[:, j * span : (j + 1) * span]
                + rs_in[g, 0, i, :, at : at + span].astype(F32)
                + rs_in[g, 1, i, :, at : at + span].astype(F32)
            )
            out_ref[:, cols] = (middle[mine, cols].astype(F32) + down_sum).astype(BF16)

    steps = (contract, outward, onward, finish)
    for t in range(len(groups) + len(steps) - 1):
        for k, step in enumerate(steps):
            if 0 <= t - k < len(groups):
                step(t - k)

    for g in range(len(groups)):
        swap_of(g).wait_send()
        for i in range(6):
            send_of(g, i).wait_send()
    wos.gone()
    ats.gone()
    for item in ITEMS:
        kv_prev(item).wait_send()
        kv_right(item, last).wait_send()
        kv_left(item, last).wait_send()

        @pl.when((y == 1) | (y == 2))
        def _():
            kv_relay_right(item).wait_send()
            kv_relay_left(item).wait_send()

    stream.gone()


def local(n_sp, n_tp, residual, queries, keys, values, gate_cache, doc_ids, out_weight, mix_gain, gate_weight, up_weight, down_weight):
    tok, width = queries.shape
    d_model = out_weight.shape[1]
    rows = tok // n_tp
    wr, ff = gate_weight.shape
    heads = gate_cache.shape[1]
    nz = n_sp // NY
    hz = nz // 2
    tile = 128
    early = 9 * 128
    span = d_model // nz
    n_groups = nz // 4
    vmem = pl.BlockSpec(memory_space=pltpu.VMEM)
    anywhere = pl.BlockSpec(memory_space=pl.ANY)
    dma = pltpu.SemaphoreType.DMA
    return pl.pallas_call(
        functools.partial(kernel, n_sp, n_tp),
        out_shape=jax.ShapeDtypeStruct((rows, d_model), BF16),
        in_specs=[vmem, *[anywhere] * 3, vmem, *[anywhere] * 5, vmem],
        out_specs=vmem,
        scratch_shapes=[
            pltpu.VMEM(((REACH + 1) * tok, width), BF16),
            pltpu.VMEM(((REACH + 1) * tok, width), BF16),
            pltpu.VMEM((8, (REACH + 1) * tok), F32),
            pltpu.VMEM((tok, heads), F32),
            pltpu.VMEM((ff, wr), BF16),
            pltpu.VMEM((n_sp, wr, early), BF16),
            pltpu.VMEM((n_sp, wr, 3 * ff - early), BF16),
            pltpu.VMEM((n_tp, width, d_model), BF16),
            pltpu.VMEM((tok, d_model), BF16),
            pltpu.VMEM((tile, REACH * tok + tile), F32),
            pltpu.VMEM((tok, 128), F32),
            pltpu.VMEM((tok, n_tp * width), BF16),
            pltpu.VMEM((n_groups, n_tp // 2, 2, rows, 4 * span), BF16),
            pltpu.VMEM((n_groups, n_tp // 2, rows, 4 * span), BF16),
            pltpu.VMEM((n_groups, 6, rows, 2 * span), BF16),
            pltpu.VMEM((rows, 4 * span), F32),
            pltpu.VMEM((n_groups, 2, rows, 2 * span), BF16),
            pltpu.VMEM((n_groups, 2, 2, rows, 2 * span), BF16),
            pltpu.VMEM((tok, d_model), BF16),
            pltpu.VMEM((tok, ff), BF16),
            pltpu.VMEM((tok, d_model), BF16),
            dma((6 + ff // 64,)),
            dma((3, 5)),
            dma((3, 4)),
            dma((1, 2, hz + 1)),
            dma((1, 2, hz + 1)),
            dma((1, 3, nz)),
            dma((1, 3, nz)),
            dma((1, 3)),
            dma((1, 3)),
            dma((1, 2, hz + 1, 2)),
            dma((1, 2, hz + 1, 2)),
            dma((n_groups, 7)),
            dma((n_groups, 7)),
            dma((8, 4)),
            dma((8, 4)),
            dma((8, tok // tile)),
            dma((8, tok // tile)),
        ],
        compiler_params=pltpu.CompilerParams(
            collective_id=0, has_side_effects=True, vmem_limit_bytes=60 * 1024 * 1024
        ),
    )(
        queries, keys, values, gate_cache, doc_ids[None], gate_weight, up_weight, down_weight, out_weight, residual, mix_gain[None]
    )


def solution(mesh):
    n_sp, n_tp = mesh.shape["sp"], mesh.shape["tp"]
    return jax.shard_map(
        functools.partial(local, n_sp, n_tp),
        mesh=mesh,
        in_specs=(
            P("sp", None), P("sp", "tp"), P("sp", "tp"), P("sp", "tp"), P("sp", "tp"), P("sp"),
            P("tp", None), P(), P("sp", "tp"), P("sp", "tp"), P("tp", "sp"),
        ),
        out_specs=P(("sp", "tp"), None),
        check_vma=False,
    )
```
